128 devices in a mesh: ep: 16 (over z, x), tp: 8 (over y, core).
Axes of the slice: x: 4, y: 4, z: 4, core: 2. Of those that a mesh axis runs over, the one named last changes fastest.
Arguments:
- tokens: bfloat16 [4096, 2048], P('ep'), may hold values from -40 to 40
- cotangent: bfloat16 [4096, 2048], P('ep'), may hold values from -6 to 6
- expert_ids: int32 [4096, 4], P('ep'), may hold values from 0 to 31, all different within a row; in each aligned block of 256 rows (0 to 255, 256 to 511, ...) at most 48 rows name the same one
- route_weights: bfloat16 [4096, 4], P('ep'), may hold values from 0.099609375 to 1
- gate_weight: bfloat16 [32, 2048, 2048], P('ep', None, 'tp'), may hold values from -0.125 to 0.125
- up_weight: bfloat16 [32, 2048, 2048], P('ep', None, 'tp'), may hold values from -0.125 to 0.125
- down_weight: bfloat16 [32, 2048, 2048], P('ep', 'tp'), may hold values from -0.125 to 0.125
- dense_weight: bfloat16 [2048, 2048], P('tp', 'ep'), may hold values from -0.125 to 0.125
- dense_gate: float32 [2048], replicated, may hold values from 0.1 to 1.9
Outputs:
- token_grad: bfloat16 [4096, 2048], P('ep', 'tp')
- weight_grad: bfloat16 [4096, 4], P('ep')
- gate_grad: float32 [32, 2048, 2048], P('ep', None, 'tp')
- up_grad: float32 [32, 2048, 2048], P('ep', None, 'tp')
- down_grad: float32 [32, 2048, 2048], P('ep', 'tp')
- dense_grad: float32 [2048, 2048], P('tp', 'ep')
The draws below stay inside these ranges and needn't reach their ends.
Inputs may be any that keep to these rules, and one draw needn't show every extreme that they name: `expert_ids`: in the rows of one device, at most 48 routed rows name any one expert, and in every draw some expert is named by exactly 48 rows of some device.
All inputs are finite; a program needn't handle non-finite values.
Results may differ from the reference program's by a relative error of at most 0.02.
Values may be sent and summed in bfloat16 or wider, within the bound.
A program may use at most 128 MiB of HBM per device.

```python
import math
import jax
import jax.numpy as jnp
import numpy as np
from jax import lax

D = 2048
FF = 2048
TOP_K = 4
TOK_DEV = 256
EXPERTS = 32
TOKENS = 4096
CAP = 48
N_EP = 16
N_TP = 8


def draw_tokens(key, part):
    key_scale = jax.random.fold_in(key, 11)
    key_base = jax.random.fold_in(key, 12)
    row_scale = jnp.exp(jax.random.uniform(key_scale, (TOKENS, 1), jnp.float32, math.log(0.5), math.log(6.0)))
    values = jax.random.normal(key_base, (TOKENS, D), jnp.float32)
    return jnp.clip(values * row_scale, -40.0, 40.0).astype(jnp.bfloat16)


def with_spikes(result, stream_key, source, target, blocks, factor):
    def block_of(axis_at):
        return (jnp.arange(result.shape[axis_at]) // (result.shape[axis_at] // blocks)).reshape((-1,) + (1,) * (result.ndim - 1 - axis_at))

    first = jax.random.permutation(stream_key, blocks)[block_of(target)]
    second = (block_of(target) + blocks // 2) % blocks
    return jnp.where((block_of(source) == first) | (block_of(source) == second), factor * result, result)


def block_levels(own_key, shape, cuts, least, top_value):
    level = 1.0
    for dim, blocks in cuts:
        steps = jax.random.uniform(jax.random.fold_in(jax.random.fold_in(own_key, 6), dim), (blocks,), jnp.float32, least / len(cuts), top_value / len(cuts))
        level = level * jnp.repeat(jnp.exp(steps), shape[dim] // blocks).reshape((-1,) + (1,) * (len(shape) - 1 - dim))
    return level


def routed_block(key, own, number, rows, number_of, top, bound, lean):
    sequence = jax.random.permutation(key, number_of)
    heavy_load, common = load_shares(number_of, rows * top, bound, lean, True), load_shares(number_of, rows * top, bound, lean, False)
    places = jnp.arange(number_of)

    def named(tallies, offset_by):
        used = int((tallies > 0).sum())
        fixed = max(1, used // 4)
        moved = fixed + (places - fixed + offset_by * (used - fixed)) % max(1, number_of - fixed)
        return jnp.zeros((number_of,), jnp.int32).at[sequence[jnp.where(places < fixed, places, moved)]].set(jnp.asarray(tallies, jnp.int32))

    tallies = jnp.where(number % 4 == 0, named(heavy_load, number // 4), named(common, number - number // 4 - 1))
    mixed = jax.random.permutation(jax.random.fold_in(own, 3), number_of)
    source_of, taker = mixed[0:number_of // 2 * 2:2], mixed[1:number_of // 2 * 2:2]
    margin = jnp.minimum(tallies[source_of] - 1, bound - tallies[taker]) // 2
    margin = jnp.where((source_of == sequence[0]) | (taker == sequence[0]) | (tallies[taker] == 0), 0, jnp.maximum(margin, 0))
    moved = jax.random.randint(jax.random.fold_in(own, 4), (number_of // 2,), 0, 1 << 20) % (margin + 1)
    tallies = tallies.at[source_of].add(-moved).at[taker].add(moved)
    labels = jnp.searchsorted(jnp.cumsum(tallies), jnp.arange(rows * top), side="right").astype(jnp.int32)
    listing = labels.reshape(top, rows).T
    listing = listing[jax.random.permutation(jax.random.fold_in(own, 1), rows)]
    offset_by = jax.random.randint(jax.random.fold_in(own, 2), (rows, 1), 0, top)
    return jnp.take_along_axis(listing, (jnp.arange(top)[None, :] + offset_by) % top, axis=1)


def load_shares(count, total, most, skew, full):
    loads = [(1 << 20) // math.isqrt(grade ** skew) + 1 for grade in range(1, count + 1)]
    largest = most if full else min(most, max(-(-total // count), total * loads[0] // sum(loads)))
    least = 1 if total - largest >= count - 1 else 0
    given, surplus = [largest] + [least] * (count - 1), total - largest - least * (count - 1)
    while surplus > 0:
        candidates = [i for i in range(1, count) if given[i] < largest] or [i for i in range(1, count) if given[i] < most]
        whole, remaining = sum([loads[i] for i in candidates]), surplus
        for i in candidates:
            extra = min(most - given[i], max(1, remaining * loads[i] // whole), surplus)
            given[i] = given[i] + extra
            surplus = surplus - extra
    return np.array(given)


def noise(own_key, extent, width, limit, cuts=(), kind=jnp.bfloat16):
    result = width * jax.random.normal(own_key, extent, jnp.float32)
    if cuts:
        result = result * block_levels(own_key, extent, cuts, -0.22, 0.18)
    return jnp.clip(result, -limit, limit).astype(kind)


def gaussian_with(own_key, shape, deviation, most, cuts, heavy, kind=jnp.bfloat16):
    result = deviation * jax.random.normal(own_key, shape, jnp.float32)
    if cuts:
        result = result * block_levels(own_key, shape, cuts, -0.22, 0.18)
    return jnp.clip(with_spikes(result, jax.random.fold_in(own_key, 3), *heavy), -most, most).astype(kind)


def setup_inputs(seed: int = 0) -> dict:
    splits = jax.random.split(jax.random.key(seed), 10)
    tokens = draw_tokens(jax.random.fold_in(splits[9], 71), 0)
    cotangent = gaussian_with(splits[1], (TOKENS, D), 1.0, 6.0, ((0, 16),), (0, 1, 16, 2.0))
    expert_ids_keys = jax.random.split(jax.random.fold_in(splits[2], 1), TOKENS // TOK_DEV)
    expert_ids_turns = jax.random.permutation(jax.random.fold_in(splits[2], 3), TOKENS // TOK_DEV)
    expert_ids = jax.vmap(lambda own, number: routed_block(jax.random.fold_in(splits[2], 2), own, number, TOK_DEV, EXPERTS, TOP_K, CAP, 2))(expert_ids_keys, expert_ids_turns).reshape((TOKENS, TOP_K))
    route_weights = jnp.clip(0.099609375 + 0.9003906 * jax.random.uniform(splits[3], (TOKENS, TOP_K), jnp.float32) ** block_levels(splits[3], (TOKENS, TOP_K), ((0, 16),), -0.2, 0.2), 0.099609375, 1.0).astype(jnp.bfloat16)
    gate_weight = noise(splits[4], (EXPERTS, D, FF), D ** -0.5, 0.125, ((0, 16), (2, 8)))
    up_weight = noise(splits[5], (EXPERTS, D, FF), D ** -0.5, 0.125, ((0, 16), (2, 8)))
    down_weight = noise(splits[6], (EXPERTS, FF, D), FF ** -0.5, 0.125, ((0, 16), (1, 8)))
    dense_weight = noise(splits[7], (D, D), D ** -0.5, 0.125, ((0, 8), (1, 16)))
    dense_gate = jnp.clip(1.0 + 0.18 * jax.random.normal(splits[8], (D,), jnp.float32), 0.1, 1.9)
    return dict(tokens=tokens, cotangent=cotangent, expert_ids=expert_ids, route_weights=route_weights, gate_weight=gate_weight, up_weight=up_weight, down_weight=down_weight, dense_weight=dense_weight, dense_gate=dense_gate)


clamp_limit = 7.0
sigmoid_slope = 1.702


def rounded(value):
    return lax.optimization_barrier(value.astype(jnp.bfloat16)).astype(jnp.float32)


def expert_back(row_input, row_cotan, row_weight, w_gate, w_up, w_down):
    gate_pre = jnp.dot(row_input, w_gate, preferred_element_type=jnp.float32)
    up_pre = jnp.dot(row_input, w_up, preferred_element_type=jnp.float32)
    gate_val = jnp.minimum(gate_pre, clamp_limit)
    up_val = jnp.clip(up_pre, -clamp_limit, clamp_limit)
    squash = jax.nn.sigmoid(sigmoid_slope * gate_val)
    hidden = ((up_val + 1.0) * gate_val * squash).astype(jnp.bfloat16)
    down_back = lax.dot_general(row_cotan, w_down, (((1,), (1,)), ((), ())), preferred_element_type=jnp.float32)
    scores = jnp.sum(hidden.astype(jnp.float32) * down_back, axis=1)
    scale_col = row_weight.astype(jnp.float32)[:, None]
    hidden_back = scale_col * down_back
    gate_slope = squash + sigmoid_slope * gate_val * squash * (1.0 - squash)
    gate_back = jnp.where(gate_pre < clamp_limit, hidden_back * (up_val + 1.0) * gate_slope, 0.0).astype(jnp.bfloat16)
    up_back = jnp.where(jnp.abs(up_pre) < clamp_limit, hidden_back * gate_val * squash, 0.0).astype(jnp.bfloat16)
    weighted = (scale_col * row_cotan.astype(jnp.float32)).astype(jnp.bfloat16)
    input_back = lax.dot_general(gate_back, w_gate, (((1,), (1,)), ((), ())), preferred_element_type=jnp.float32)
    input_back = input_back + lax.dot_general(up_back, w_up, (((1,), (1,)), ((), ())), preferred_element_type=jnp.float32)
    grad_gate = lax.dot_general(row_input, gate_back, (((0,), (0,)), ((), ())), preferred_element_type=jnp.float32)
    grad_up = lax.dot_general(row_input, up_back, (((0,), (0,)), ((), ())), preferred_element_type=jnp.float32)
    grad_down = lax.dot_general(hidden, weighted, (((0,), (0,)), ((), ())), preferred_element_type=jnp.float32)
    return input_back, scores, grad_gate, grad_up, grad_down


def reference(tokens, cotangent, expert_ids, route_weights, gate_weight, up_weight, down_weight, dense_weight, dense_gate):
    routed = TOKENS * TOP_K
    flat_ids = expert_ids.reshape(routed).astype(jnp.int32)
    sorted_rows = jnp.argsort(flat_ids, stable=True).astype(jnp.int32)
    onehot = (flat_ids[:, None] == jnp.arange(EXPERTS, dtype=jnp.int32)[None, :]).astype(jnp.int32)
    counts = jnp.sum(onehot, axis=0).astype(jnp.int32)
    starts = (jnp.cumsum(counts) - counts).astype(jnp.int32)
    longest = N_EP * CAP
    flat_weights = route_weights.reshape(routed)
    unit_block = FF // N_TP

    def one_expert(expert):
        offsets = jnp.arange(longest, dtype=jnp.int32)
        in_use = offsets < counts[expert]
        row_ids = sorted_rows[jnp.minimum(starts[expert] + offsets, routed - 1)]
        owners = (row_ids // TOP_K).astype(jnp.int32)
        bf_zero = jnp.zeros((), jnp.bfloat16)
        row_input = jnp.where(in_use[:, None], tokens[owners], bf_zero)
        row_cotan = jnp.where(in_use[:, None], cotangent[owners], bf_zero)
        row_weight = jnp.where(in_use, flat_weights[row_ids], bf_zero)
        back_sum = jnp.zeros((longest, D), jnp.float32)
        score_sum = jnp.zeros((longest,), jnp.float32)
        gate_parts, up_parts, down_parts = [], [], []
        for segment in range(N_TP):
            low = segment * unit_block
            high = low + unit_block
            pieces_out = expert_back(row_input, row_cotan, row_weight, gate_weight[expert][:, low:high],
                                     up_weight[expert][:, low:high], down_weight[expert][low:high, :])
            back_sum = back_sum + rounded(pieces_out[0])
            score_sum = score_sum + rounded(pieces_out[1])
            gate_parts.append(pieces_out[2])
            up_parts.append(pieces_out[3])
            down_parts.append(pieces_out[4])
        targets = jnp.where(in_use, row_ids, routed).astype(jnp.int32)
        return (back_sum.astype(jnp.bfloat16), score_sum, targets, jnp.concatenate(gate_parts, axis=1),
                jnp.concatenate(up_parts, axis=1), jnp.concatenate(down_parts, axis=0))

    backs, scores, targets, gate_grad, up_grad, down_grad = lax.map(one_expert, jnp.arange(EXPERTS, dtype=jnp.int32))
    flat_targets = targets.reshape(EXPERTS * longest)
    flat_back = jnp.zeros((routed + 1, D), jnp.float32).at[flat_targets].add(backs.reshape(EXPERTS * longest, D).astype(jnp.float32))
    flat_score = jnp.zeros((routed + 1,), jnp.float32).at[flat_targets].add(scores.reshape(EXPERTS * longest))
    gated_cotan = (dense_gate[None, :] * cotangent.astype(jnp.float32)).astype(jnp.bfloat16)
    dense_back = lax.dot_general(gated_cotan, dense_weight, (((1,), (1,)), ((), ())), preferred_element_type=jnp.float32)
    dense_grad = lax.dot_general(tokens, gated_cotan, (((0,), (0,)), ((), ())), preferred_element_type=jnp.float32)
    token_grad = (jnp.sum(flat_back[:routed].reshape(TOKENS, TOP_K, D), axis=1) + dense_back).astype(jnp.bfloat16)
    weight_grad = flat_score[:routed].reshape(TOKENS, TOP_K).astype(jnp.bfloat16)
    return token_grad, weight_grad, gate_grad, up_grad, down_grad, dense_grad
```

```python
import functools

import jax
import jax.numpy as jnp
from jax import lax
from jax.experimental import pallas as pl
from jax.experimental.pallas import tpu as pltpu
from jax.sharding import PartitionSpec as P

clamp_limit = 7.0
sigmoid_slope = 1.702
MESH = pl.DeviceIdType.MESH
BF = jnp.bfloat16
F32 = jnp.float32
SIDE = 4


def place():
    ep, tp = lax.axis_index("ep"), lax.axis_index("tp")
    return ep, tp, tp // 2, lax.rem(tp, 2)


def shifted(ep, d, sign):
    z, x = ep // SIDE, lax.rem(ep, SIDE)
    dz, dx = d // SIDE, lax.rem(d, SIDE)
    if sign < 0:
        dz, dx = SIDE - dz, SIDE - dx
    return lax.rem(z + dz, SIDE) * SIDE + lax.rem(x + dx, SIDE)


def tp_at(y, c):
    return lax.rem(y, 4) * 2 + c


def greet(devices):
    barrier = pltpu.get_barrier_semaphore()
    for device in devices:
        pl.semaphore_signal(barrier, inc=1, device_id=device, device_id_type=MESH)
    pl.semaphore_wait(barrier, len(devices))


def remote(src, dst, send, recv, device):
    return pltpu.make_async_remote_copy(
        src_ref=src, dst_ref=dst, send_sem=send, recv_sem=recv, device_id=device, device_id_type=MESH
    )


def dispatch_kernel(
    n, rows_ref, wsend_ref, dw_ref, r_ref, rw_ref, dwall_ref,
    a_send, a_recv, w_send, w_recv, b_send, b_recv, y_send, y_recv, o_send, o_recv, q_send, q_recv, local,
):
    ep, tp, y, c = place()
    half = rows_ref.shape[3]
    width = dw_ref.shape[1]
    par = lax.rem(y, 2)
    cols = pl.ds(pl.multiple_of(c * half, half), half)
    up, down, mate = (ep, tp_at(y + 1, c)), (ep, tp_at(y + 3, c)), (ep, tp_at(y, 1 - c))
    greet([(shifted(ep, d, 1), tp) for d in range(1, n)] + [up, down, mate])

    def a_copy(d):
        return remote(
            rows_ref.at[shifted(ep, d, 1)], r_ref.at[par, :, ep, :, cols],
            a_send.at[d], a_recv.at[d], (shifted(ep, d, 1), tp),
        )

    def w_copy(d):
        return remote(
            wsend_ref.at[shifted(ep, d, 1)], rw_ref.at[ep], w_send.at[d], w_recv.at[d], (shifted(ep, d, 1), tp)
        )

    def b_copy(d):
        return remote(
            dw_ref, dwall_ref.at[:, pl.ds(pl.multiple_of(ep * width, width), width)],
            b_send.at[d], b_recv.at[d], (shifted(ep, d, 1), tp),
        )

    own_rows = pltpu.make_async_copy(rows_ref.at[ep], r_ref.at[par, :, ep, :, cols], local.at[0])
    own_weight = pltpu.make_async_copy(wsend_ref.at[ep], rw_ref.at[ep], local.at[1])
    own_dense = pltpu.make_async_copy(
        dw_ref, dwall_ref.at[:, pl.ds(pl.multiple_of(ep * width, width), width)], local.at[2]
    )
    own_rows.start()
    own_weight.start()
    own_dense.start()

    @pl.loop(1, n)
    def _(d):
        a_copy(d).start()

    @pl.loop(1, n)
    def _(d):
        w_copy(d).start()
        b_copy(d).start()

    own_rows.wait()
    own_weight.wait()
    own_dense.wait()

    def y_copy(d, e):
        s = shifted(ep, d, -1)
        part = r_ref.at[par, e, s, :, cols]
        return remote(part, part, y_send.at[e, d], y_recv.at[e, d], up if e == 0 else down)

    def o_copy(d):
        part = r_ref.at[par, :, shifted(ep, d, -1), :, cols]
        return remote(part, part, o_send.at[d], o_recv.at[d], mate)

    def q_copy(d, e):
        part = r_ref.at[1 - par, e, shifted(ep, d, -1), :, cols]
        return remote(part, part, q_send.at[e, d], q_recv.at[e, d], mate)

    lag = 3

    @pl.loop(0, n + lag)
    def _(t):
        @pl.when(t < n)
        def _():
            @pl.when(t > 0)
            def _():
                a_copy(t).wait_recv()

            y_copy(t, 0).start()
            y_copy(t, 1).start()
            o_copy(t).start()

        @pl.when(t >= lag)
        def _():
            for e in range(2):
                y_copy(t - lag, e).wait_recv()
                q_copy(t - lag, e).start()

    @pl.loop(0, n)
    def _(d):
        @pl.when(d > 0)
        def _():
            a_copy(d).wait_send()
            w_copy(d).wait()
            b_copy(d).wait()

        o_copy(d).wait()
        for e in range(2):
            y_copy(d, e).wait_send()
            q_copy(d, e).wait()


def dispatch(rows, wsend, dw, n):
    slots = rows.shape[2]
    model = rows.shape[3] * 2
    dma = pltpu.SemaphoreType.DMA
    return pl.pallas_call(
        functools.partial(dispatch_kernel, n),
        out_shape=(
            jax.ShapeDtypeStruct((2, 2, n, slots, model), BF),
            jax.ShapeDtypeStruct(wsend.shape, BF),
            jax.ShapeDtypeStruct((dw.shape[0], dw.shape[1] * n), BF),
        ),
        in_specs=[pl.BlockSpec(memory_space=pl.ANY)] * 3,
        out_specs=[pl.BlockSpec(memory_space=pl.ANY)] * 3,
        scratch_shapes=[
            dma((n,)), dma((n,)), dma((n,)), dma((n,)), dma((n,)), dma((n,)),
            dma((2, n)), dma((2, n)), dma((n,)), dma((n,)), dma((2, n)), dma((2, n)), dma((3,)),
        ],
        compiler_params=pltpu.CompilerParams(collective_id=0, has_side_effects=True),
    )(rows, wsend, dw)


def combine_kernel(
    n, rb_ref, sc_ref, dg_ref, hl_ref, hs_ref, dgall_ref,
    own, mine, yin, tot,
    l_sem, d_send, d_recv, y_send, y_recv, t_send, t_recv, s_send, s_recv, g_send, g_recv, local,
):
    ep, tp, y, c = place()
    block = rb_ref.shape[3] // 8
    width = dgall_ref.shape[2]
    up, down, mate = (ep, tp_at(y + 1, c)), (ep, tp_at(y + 3, c)), (ep, tp_at(y, 1 - c))
    greet([(shifted(ep, d, 1), tp) for d in range(1, n)] + [up, down, mate])

    def at_block(index):
        return pl.ds(pl.multiple_of(index * block, block), block)

    def own_copy(d, j):
        return pltpu.make_async_copy(
            rb_ref.at[:, shifted(ep, d, 1), :, at_block(2 * j + c)], own.at[d, :, :, at_block(j)], l_sem.at[j, d]
        )

    def mate_copy(d, j):
        return remote(
            rb_ref.at[:, shifted(ep, d, 1), :, at_block(2 * j + 1 - c)], mine.at[d, :, :, at_block(j)],
            d_send.at[j, d], d_recv.at[j, d], mate,
        )

    def s_copy(d):
        return remote(sc_ref.at[shifted(ep, d, 1)], hs_ref.at[ep], s_send.at[d], s_recv.at[d], (shifted(ep, d, 1), tp))

    def g_copy(d):
        to = shifted(ep, d, 1)
        return remote(
            dg_ref.at[:, pl.ds(pl.multiple_of(to * width, width), width)], dgall_ref.at[ep],
            g_send.at[d], g_recv.at[d], (to, tp),
        )

    own_score = pltpu.make_async_copy(sc_ref.at[ep], hs_ref.at[ep], local.at[0])
    own_dense = pltpu.make_async_copy(
        dg_ref.at[:, pl.ds(pl.multiple_of(ep * width, width), width)], dgall_ref.at[ep], local.at[1]
    )
    own_score.start()
    own_dense.start()

    @pl.loop(0, n)
    def _(d):
        for j in range(4):
            mate_copy(d, j).start()
            own_copy(d, j).start()

    @pl.loop(1, n)
    def _(d):
        s_copy(d).start()
        g_copy(d).start()

    def y_copy(d, way):
        index = lax.rem(y + 1, 4) if way == 0 else lax.rem(y + 3, 4)
        return remote(
            own.at[d, :, :, at_block(index)], yin.at[way, d], y_send.at[way, d], y_recv.at[way, d],
            up if way == 0 else down,
        )

    def t_copy(d):
        return remote(tot.at[d], hl_ref.at[ep], t_send.at[d], t_recv.at[d], (shifted(ep, d, 1), tp))

    lag = 4

    @pl.loop(0, n + lag)
    def _(t):
        @pl.when(t < n)
        def _():
            for j in range(4):
                own_copy(t, j).wait()
                mate_copy(t, j).wait_recv()
            for e in range(2):
                own[t, e] = (own[t, e].astype(F32) + mine[t, e].astype(F32)).astype(BF)
            y_copy(t, 0).start()
            y_copy(t, 1).start()

        @pl.when(t >= lag)
        def _():
            d = t - lag
            y_copy(d, 0).wait_recv()
            y_copy(d, 1).wait_recv()
            for e in range(2):
                near = own[d, e, :, at_block(y)].astype(F32)
                near = near + yin[0, d, e].astype(F32) + yin[1, d, e].astype(F32)
                tot[d, e, :, 0:block] = near.astype(BF)
                tot[d, e, :, block : 2 * block] = own[d, e, :, at_block(lax.rem(y + 2, 4))]

            @pl.when(d > 0)
            def _():
                t_copy(d).start()

    own_tot = pltpu.make_async_copy(tot.at[0], hl_ref.at[ep], local.at[2])
    own_tot.start()
    own_score.wait()
    own_dense.wait()
    own_tot.wait()

    @pl.loop(0, n)
    def _(d):
        @pl.when(d > 0)
        def _():
            s_copy(d).wait()
            g_copy(d).wait()
            t_copy(d).wait()

        for j in range(4):
            mate_copy(d, j).wait_send()
        for way in range(2):
            y_copy(d, way).wait_send()


def combine(rb, sc, dg, n, width):
    slots, model = rb.shape[2:]
    dma = pltpu.SemaphoreType.DMA
    return pl.pallas_call(
        functools.partial(combine_kernel, n),
        out_shape=(
            jax.ShapeDtypeStruct((n, 2, slots, model // 4), BF),
            jax.ShapeDtypeStruct(sc.shape, BF),
            jax.ShapeDtypeStruct((n, dg.shape[0], width), BF),
        ),
        in_specs=[pl.BlockSpec(memory_space=pl.ANY)] * 3,
        out_specs=[pl.BlockSpec(memory_space=pl.ANY)] * 3,
        scratch_shapes=[
            pltpu.VMEM((n, 2, slots, model // 2), BF),
            pltpu.VMEM((n, 2, slots, model // 2), BF),
            pltpu.VMEM((2, n, 2, slots, model // 8), BF),
            pltpu.VMEM((n, 2, slots, model // 4), BF),
            dma((4, n)), dma((4, n)), dma((4, n)), dma((2, n)), dma((2, n)), dma((n,)), dma((n,)),
            dma((n,)), dma((n,)), dma((n,)), dma((n,)), dma((3,)),
        ],
        compiler_params=pltpu.CompilerParams(collective_id=1, has_side_effects=True),
    )(rb, sc, dg)


def finish_kernel(part_ref, score_ref, got_ref, scores_ref, p_send, p_recv, s_send, s_recv, local):
    ep, tp, y, c = place()
    greet([(ep, lax.rem(tp + k, 8)) for k in range(1, 8)])
    across = remote(part_ref, got_ref, p_send, p_recv, (ep, tp_at(y + 2, c)))
    across.start()
    own = pltpu.make_async_copy(score_ref, scores_ref.at[tp], local)
    own.start()
    copies = [
        remote(score_ref, scores_ref.at[tp], s_send.at[k], s_recv.at[k], (ep, lax.rem(tp + k, 8))) for k in range(1, 8)
    ]
    for copy in copies:
        copy.start()
    own.wait()
    for copy in copies:
        copy.wait()
    across.wait()


def finish(part, score):
    dma = pltpu.SemaphoreType.DMA
    return pl.pallas_call(
        finish_kernel,
        out_shape=(
            jax.ShapeDtypeStruct(part.shape, part.dtype),
            jax.ShapeDtypeStruct((8, *score.shape), score.dtype),
        ),
        in_specs=[pl.BlockSpec(memory_space=pltpu.VMEM)] * 2,
        out_specs=[pl.BlockSpec(memory_space=pltpu.VMEM)] * 2,
        scratch_shapes=[dma, dma, dma((8,)), dma((8,)), dma],
        compiler_params=pltpu.CompilerParams(collective_id=2, has_side_effects=True),
    )(part, score)


def batched(a, b, ca, cb):
    return lax.dot_general(a, b, (((ca,), (cb,)), ((0,), (0,))), preferred_element_type=F32)


def shards(
    tokens, cotangent, expert_ids, route_weights, gate_weight, up_weight, down_weight, dense_weight, dense_gate
):
    tok_rows, model = tokens.shape
    top_count = expert_ids.shape[1]
    local_count = gate_weight.shape[0]
    n = lax.axis_size("ep")
    experts = local_count * n
    slots = tok_rows * top_count * 3 // (2 * experts)
    half, block = model // 2, model // 8
    ep, tp, y, c = place()

    names = expert_ids.T[None] == jnp.arange(experts, dtype=jnp.int32)[:, None, None]
    member = jnp.sum(names.astype(F32), axis=1)
    weight_of = jnp.sum(jnp.where(names, route_weights.T[None].astype(F32), 0.0), axis=1)
    row_at = lax.broadcasted_iota(jnp.int32, (tok_rows, tok_rows), 0)
    col_at = lax.broadcasted_iota(jnp.int32, (tok_rows, tok_rows), 1)
    before = (row_at < col_at).astype(BF)
    rank = jnp.dot(member.astype(BF), before, preferred_element_type=F32)
    rank = jnp.where(member > 0.5, rank, -1.0)
    places = jnp.arange(slots, dtype=jnp.int32).astype(F32)
    picked = rank[:, None, :] == places[None, :, None]
    pick = picked.astype(BF)
    slot_weight = jnp.sum(jnp.where(picked, weight_of[:, None, :], 0.0), axis=2).astype(BF)
    pick_rows = pick.reshape(experts * slots, tok_rows)
    wsend = jnp.pad(slot_weight.reshape(n, local_count, slots), ((0, 0), (0, 16 - local_count), (0, 128 - slots)))

    source = jnp.where(
        lax.rem(y, 2) == 0,
        lax.dynamic_slice_in_dim(tokens, c * half, half, 1),
        lax.dynamic_slice_in_dim(cotangent, c * half, half, 1),
    )
    rows = jnp.dot(pick_rows, source, preferred_element_type=F32).astype(BF)
    rows = rows.reshape(n, local_count, slots, half)

    got, got_weight, dense_all = dispatch(rows, wsend, dense_weight, n)

    gated = (dense_gate[None, :] * cotangent.astype(F32)).astype(BF)
    own_input = lax.dynamic_slice_in_dim(tokens, tp * block, block, 1)
    dense_part = lax.dot_general(
        own_input, gated, (((0,), (0,)), ((), ())), preferred_element_type=F32
    ).astype(BF)

    row_input = got[0].reshape(local_count, n * slots, model)
    row_cotan = got[1].reshape(local_count, n * slots, model)
    row_weight = got_weight[:, :local_count, :slots].transpose(1, 0, 2).reshape(local_count, n * slots, 1).astype(F32)

    gate_pre = batched(row_input, gate_weight, 2, 1)
    up_pre = batched(row_input, up_weight, 2, 1)
    gate_val = jnp.minimum(gate_pre, clamp_limit)
    up_val = jnp.clip(up_pre, -clamp_limit, clamp_limit)
    squash = jax.nn.sigmoid(sigmoid_slope * gate_val)
    hidden = ((up_val + 1.0) * gate_val * squash).astype(BF)
    down_back = batched(row_cotan, down_weight, 2, 2)
    scores = jnp.sum(hidden.astype(F32) * down_back, axis=2)
    hidden_back = row_weight * down_back
    gate_slope = squash + sigmoid_slope * gate_val * squash * (1.0 - squash)
    gate_back = jnp.where(gate_pre < clamp_limit, hidden_back * (up_val + 1.0) * gate_slope, 0.0).astype(BF)
    up_back = jnp.where(jnp.abs(up_pre) < clamp_limit, hidden_back * gate_val * squash, 0.0).astype(BF)
    weighted = (row_weight * row_cotan.astype(F32)).astype(BF)
    back = batched(gate_back, gate_weight, 2, 2) + batched(up_back, up_weight, 2, 2)
    grad_gate = batched(row_input, gate_back, 1, 1)
    grad_up = batched(row_input, up_back, 1, 1)
    grad_down = batched(hidden, weighted, 1, 1)

    back = back.astype(BF).reshape(local_count, n, slots, model)
    score_send = jnp.pad(
        scores.astype(BF).reshape(local_count, n, slots).transpose(1, 0, 2),
        ((0, 0), (0, 16 - local_count), (0, 128 - slots)),
    )
    home, home_score, dense_parts = combine(back, score_send, dense_part, n, model // n)

    both = lax.dot_general(
        pick_rows, home.reshape(experts * slots, 2 * block), (((0,), (0,)), ((), ())), preferred_element_type=F32
    )
    slot_score = home_score[:, :local_count, :slots].reshape(experts, slots, 1).astype(F32)
    of_expert = jnp.sum(jnp.where(picked, slot_score, 0.0), axis=1)
    of_choice = jnp.sum(jnp.where(names, of_expert[:, None, :], 0.0), axis=0)
    score_part = of_choice.reshape(tok_rows * top_count // 128, 128)
    far, all_scores = finish(both[:, block:].astype(BF), score_part)

    dense_back = lax.dot_general(gated, dense_all, (((1,), (1,)), ((), ())), preferred_element_type=F32)
    token_grad = (both[:, :block] + far.astype(F32) + dense_back).astype(BF)
    weight_grad = jnp.sum(all_scores, axis=0).reshape(top_count, tok_rows).T.astype(BF)
    dense_grad = jnp.sum(dense_parts.astype(F32), axis=0)
    return token_grad, weight_grad, grad_gate, grad_up, grad_down, dense_grad


def solution(mesh):
    in_specs = (
        P("ep", None),
        P("ep", None),
        P("ep", None),
        P("ep", None),
        P("ep", None, "tp"),
        P("ep", None, "tp"),
        P("ep", "tp", None),
        P("tp", "ep"),
        P(),
    )
    out_specs = (
        P("ep", "tp"),
        P("ep", None),
        P("ep", None, "tp"),
        P("ep", None, "tp"),
        P("ep", "tp", None),
        P("tp", "ep"),
    )
    return jax.shard_map(shards, mesh=mesh, in_specs=in_specs, out_specs=out_specs, check_vma=False)
```

```python
import functools

import jax
import jax.numpy as jnp
from jax import lax
from jax.experimental import pallas as pl
from jax.experimental.pallas import tpu as pltpu
from jax.sharding import PartitionSpec as P

clamp_limit = 7.0
sigmoid_slope = 1.702
MESH = pl.DeviceIdType.MESH
BF = jnp.bfloat16
F32 = jnp.float32
SIDE = 4
ORDER = (
    (0, 0), (0, 1), (1, 0), (0, 3), (3, 0), (1, 1), (3, 3), (1, 3),
    (3, 1), (0, 2), (2, 0), (2, 2), (1, 2), (2, 1), (3, 2), (2, 3),
)
GROUP = 8
LAG = 3


def place():
    ep, tp = lax.axis_index("ep"), lax.axis_index("tp")
    return ep, tp, tp // 2, lax.rem(tp, 2)


def shifted(ep, step, sign):
    z, x = ep // SIDE, lax.rem(ep, SIDE)
    dz, dx = step
    if sign < 0:
        dz, dx = SIDE - dz, SIDE - dx
    return lax.rem(z + dz, SIDE) * SIDE + lax.rem(x + dx, SIDE)


def tp_at(y, c):
    return lax.rem(y, 4) * 2 + c


def greet(devices):
    barrier = pltpu.get_barrier_semaphore()
    for device in devices:
        pl.semaphore_signal(barrier, inc=1, device_id=device, device_id_type=MESH)
    pl.semaphore_wait(barrier, len(devices))


def remote(src, dst, send, recv, device):
    return pltpu.make_async_remote_copy(
        src_ref=src, dst_ref=dst, send_sem=send, recv_sem=recv, device_id=device, device_id_type=MESH
    )


def nn(a, b):
    return lax.dot_general(a, b, (((1,), (0,)), ((), ())), preferred_element_type=F32)


def nt(a, b):
    return lax.dot_general(a, b, (((1,), (1,)), ((), ())), preferred_element_type=F32)


def tn(a, b):
    return lax.dot_general(a, b, (((0,), (0,)), ((), ())), preferred_element_type=F32)


def exchange_kernel(
    n, rows_ref, weight_ref, wg_ref, wu_ref, wd_ref, tok_ref, cot_ref, scale_ref, dw_ref, pick_ref,
    held_ref, act_out, token_ref, home_score, dense_out,
    r, rw, wg, wu, wd, act, back, mine, part, first, second, total, home, score, scores, to_home,
    tok, cot, pick, dsend, dland, dwall,
    a_send, a_recv, w_send, w_recv, b_send, b_recv, g_send, g_recv,
    y_send, y_recv, o_send, o_recv, q_send, q_recv, d_send, d_recv, f_send, f_recv, h_send, h_recv,
    t_send, t_recv, s_send, s_recv, k_send, k_recv, load, local, out_sem,
):
    ep, tp, y, c = place()
    slots, half = rows_ref.shape[2:]
    quarter, block, width = half // 2, half // 4, dw_ref.shape[1]
    rows = GROUP * slots
    par = lax.rem(y, 2)
    up, down, mate = (ep, tp_at(y + 1, c)), (ep, tp_at(y + 3, c)), (ep, tp_at(y, 1 - c))
    others = [(ep, lax.rem(tp + k, 8)) for k in range(1, 8)]
    targets = [shifted(ep, step, 1) for step in ORDER]
    homes = [shifted(ep, step, -1) for step in ORDER]

    def columns(start, size):
        return pl.ds(pl.multiple_of(start, 128), size)

    mine_cols = columns(c * half, half)
    ep_cols = columns(ep * width, width)

    loads = [
        pltpu.make_async_copy(a, b, load.at[k])
        for k, (a, b) in enumerate(
            [
                (tok_ref.at[:, columns(tp * block, block)], tok),
                (cot_ref, cot),
                (wg_ref, wg),
                (wu_ref, wu),
                (wd_ref, wd),
                (pick_ref, pick),
                (dw_ref, dwall.at[:, ep_cols]),
                (weight_ref.at[ep], rw.at[0]),
                (rows_ref.at[ep, 0], r.at[par, 0, 0, :, mine_cols]),
                (rows_ref.at[ep, 1], r.at[par, 1, 0, :, mine_cols]),
            ]
        )
    ]
    for copy in loads:
        copy.start()
    greet([(targets[i], tp) for i in range(1, n)] + others + [up, down])

    def a_copy(e, i, to):
        return remote(
            rows_ref.at[to, e], r.at[par, e, i, :, mine_cols], a_send.at[e, i], a_recv.at[e, i], (to, tp)
        )

    def w_copy(i):
        return remote(weight_ref.at[targets[i]], rw.at[i], w_send.at[i], w_recv.at[i], (targets[i], tp))

    def b_copy(i):
        return remote(dw_ref, dwall.at[:, ep_cols], b_send.at[i], b_recv.at[i], (targets[i], tp))

    def g_copy(i):
        return remote(
            dsend.at[:, columns(targets[i] * width, width)], dland.at[i], g_send.at[i], g_recv.at[i], (targets[i], tp)
        )

    for i in range(1, n):
        w_copy(i).start()
    for e in range(2):
        for i in range(1, n):
            a_copy(e, i, targets[i]).start()
    for i in range(1, n):
        b_copy(i).start()

    loads[0].wait()
    loads[1].wait()
    cot[...] = (scale_ref[...] * cot[...].astype(F32)).astype(BF)
    for k in range(4):
        dsend[:, k * half // 2 : (k + 1) * half // 2] = tn(
            tok[...], cot[:, k * half // 2 : (k + 1) * half // 2]
        ).astype(BF)
    dland[0] = dsend[:, ep_cols]
    for i in range(1, n):
        g_copy(i).start()
    for copy in loads[2:]:
        copy.wait()
    for i in range(1, n):
        w_copy(i).wait_recv()

    def y_copy(e, i, way):
        piece = r.at[par, e, i, :, columns(c * half + way * quarter, quarter)]
        return remote(piece, piece, y_send.at[way, e, i], y_recv.at[way, e, i], up if way == 0 else down)

    def o_copy(e, i):
        piece = r.at[par, e, i, :, mine_cols]
        return remote(piece, piece, o_send.at[e, i], o_recv.at[e, i], mate)

    def q_copy(e, i, way):
        piece = r.at[1 - par, e, i, :, columns(c * half + way * quarter, quarter)]
        return remote(piece, piece, q_send.at[way, e, i], q_recv.at[way, e, i], mate)

    def serve(t):
        @pl.when(t < 2 * n)
        def _():
            e, i = t // n, lax.rem(t, n)

            @pl.when(i > 0)
            def _():
                a_copy(e, i, targets[1]).wait_recv()

            y_copy(e, i, 0).start()
            y_copy(e, i, 1).start()
            o_copy(e, i).start()

        @pl.when(t >= LAG)
        def _():
            e, i = (t - LAG) // n, lax.rem(t - LAG, n)
            for way in range(2):
                y_copy(e, i, way).wait_recv()
                q_copy(e, i, way).start()

    def group(q):
        return q // 2, pl.ds(lax.rem(q, 2) * GROUP, GROUP)

    def ready(q):
        e = q // 2

        @pl.loop(0, GROUP)
        def _(k):
            i = lax.rem(q, 2) * GROUP + k
            o_copy(e, i).wait_recv()
            for way in range(2):
                q_copy(e, i, way).wait_recv()

    diagonal = lax.broadcasted_iota(jnp.int32, (slots, 128), 0) == lax.broadcasted_iota(jnp.int32, (slots, 128), 1)

    def expert_rows(q):
        e, who = group(q)
        x = r[0, e, who].reshape(rows, 2 * half)
        cotan = r[1, e, who].reshape(rows, 2 * half)
        gate_pre = nn(x, wg[e])
        up_pre = nn(x, wu[e])
        down_back = nt(cotan, wd[e])
        lanes = jnp.where(e == 0, rw[who, 0, :], rw[who, 1, :])
        weight = jnp.sum(jnp.where(diagonal[None], lanes[:, None, :], 0.0), axis=2, keepdims=True).reshape(rows, 1)
        gate_val = jnp.minimum(gate_pre, clamp_limit)
        up_val = jnp.clip(up_pre, -clamp_limit, clamp_limit)
        squash = jax.nn.sigmoid(sigmoid_slope * gate_val)
        swish = gate_val * squash
        hidden = ((up_val + 1.0) * swish).astype(BF).astype(F32)
        row_score = jnp.sum(hidden * down_back, axis=1, keepdims=True).reshape(GROUP, slots, 1)
        score[pl.ds(pl.multiple_of(q * GROUP, GROUP), GROUP), :] = jnp.sum(
            jnp.where(diagonal[None], row_score, 0.0), axis=1
        )
        hidden_back = weight * down_back
        slope = squash + sigmoid_slope * swish * (1.0 - squash)
        act[0, q] = (weight * hidden).astype(BF)
        act[1, q] = jnp.where(gate_pre < clamp_limit, hidden_back * (up_val + 1.0) * slope, 0.0).astype(BF)
        act[2, q] = jnp.where(jnp.abs(up_pre) < clamp_limit, hidden_back * swish, 0.0).astype(BF)
        for k in range(4):
            cols = pl.ds(k * half // 2, half // 2)
            value = nt(act[1, q], wg[e, cols, :]) + nt(act[2, q], wu[e, cols, :])
            back[q, :, cols] = value.astype(BF)

    def d_copy(q, j):
        return remote(
            back.at[q, :, columns((2 * j + 1 - c) * block, block)], mine.at[q, :, pl.ds(j * block, block)],
            d_send.at[j, q], d_recv.at[j, q], mate,
        )

    def f_copy(q, way):
        start = lax.rem(y + 2, 4) * block + way * (block // 2)
        return remote(
            part.at[q, :, columns(start, block // 2)], first.at[way, q], f_send.at[way, q], f_recv.at[way, q],
            up if way == 0 else down,
        )

    def h_copy(q, way):
        start = lax.rem(y + (1 if way == 0 else 3), 4) * block
        return remote(
            part.at[q, :, columns(start, block)], second.at[way, q], h_send.at[way, q], h_recv.at[way, q],
            up if way == 0 else down,
        )

    def t_copy(q, k, to):
        i = lax.rem(q, 2) * GROUP + k
        return remote(
            total.at[q, pl.ds(k * slots, slots)], home.at[ep, q // 2], t_send.at[q, k], t_recv.at[q, k], (to, tp)
        )

    def own_total(e):
        return pltpu.make_async_copy(total.at[2 * e, pl.ds(0, slots)], home.at[ep, e], local.at[e])

    def core_sum(q):
        for j in range(4):
            d_copy(q, j).wait_recv()
        for j in range(4):
            cols = pl.ds(j * block, block)
            both = back[q, :, columns((2 * j + c) * block, block)].astype(F32) + mine[q, :, cols].astype(F32)
            part[q, :, cols] = both.astype(BF)
        for way in range(2):
            f_copy(q, way).start()

    def ring_sum(q):
        for way in range(2):
            f_copy(q, way).wait_recv()
        for way in range(2):
            start = lax.rem(y + (1 if way == 0 else 3), 4) * block + way * (block // 2)
            cols = columns(start, block // 2)
            part[q, :, cols] = (part[q, :, cols].astype(F32) + first[way, q].astype(F32)).astype(BF)
        for way in range(2):
            h_copy(q, way).start()

    def home_sum(q):
        for way in range(2):
            h_copy(q, way).wait_recv()
        value = part[q, :, columns(y * block, block)].astype(F32)
        total[q] = (value + second[0, q].astype(F32) + second[1, q].astype(F32)).astype(BF)
        for k in range(GROUP):
            to = jnp.where(lax.rem(q, 2) == 0, homes[k], homes[GROUP + k])
            if k == 0:

                @pl.when(lax.rem(q, 2) == 0)
                def _():
                    own_total(q // 2).start()

                @pl.when(lax.rem(q, 2) == 1)
                def _():
                    t_copy(q, 0, homes[GROUP]).start()

            else:
                t_copy(q, k, to).start()

    def held_copy(a, e):
        return pltpu.make_async_copy(r.at[a, e], held_ref.at[a, e], out_sem.at[a, e])

    def act_copy(q):
        return pltpu.make_async_copy(act.at[:, q], act_out.at[:, q], out_sem.at[2, q])

    def score_copy(k):
        return remote(score, scores.at[tp], s_send.at[k], s_recv.at[k], (ep, lax.rem(tp + k, 8)))

    def k_copy(i):
        return remote(to_home.at[i], home_score.at[ep], k_send.at[i], k_recv.at[i], (homes[i], tp))

    @pl.loop(0, 7)
    def _(q):
        start = jnp.where(q == 0, 0, jnp.minimum(q * GROUP + 2 * LAG, 2 * n + LAG))
        stop = jnp.where(q >= 3, 2 * n + LAG, (q + 1) * GROUP + 2 * LAG)
        start = jnp.where(q >= 4, 2 * n + LAG, start)
        pl.loop(start, stop)(serve)

        @pl.when((q >= 1) & (q < 5))
        def _():
            core_sum(q - 1)

        @pl.when((q >= 2) & (q < 6))
        def _():
            ring_sum(q - 2)

        @pl.when(q >= 3)
        def _():
            home_sum(q - 3)

        @pl.when(q < 4)
        def _():
            ready(q)
            expert_rows(q)
            for j in range(4):
                d_copy(q, j).start()
            act_copy(q).start()

            @pl.when(lax.rem(q, 2) == 1)
            def _():
                held_copy(0, q // 2).start()
                held_copy(1, q // 2).start()

        @pl.when(q == 3)
        def _():
            for k in range(1, 8):
                score_copy(k).start()
            scores[tp] = score[...]

        @pl.when(q == 4)
        def _():
            for k in range(1, 8):
                score_copy(k).wait_recv()
            every = scores[0]
            for k in range(1, 8):
                every = every + scores[k]
            lower = lax.broadcasted_iota(jnp.int32, (8, 128), 0) == 0
            for i in range(n):
                to_home[i] = jnp.where(lower, every[i : i + 1, :], every[n + i : n + i + 1, :])
            pltpu.make_async_copy(to_home.at[0], home_score.at[ep], local.at[2]).start()
            for i in range(1, n):
                k_copy(i).start()

    for i in range(1, n):
        b_copy(i).wait()
        g_copy(i).wait()
    dense = dland[0].astype(F32)
    for i in range(1, n):
        dense = dense + dland[i].astype(F32)
    dense_out[...] = dense
    back_dense = nt(cot[...], dwall[...])

    own_total(0).wait()
    own_total(1).wait()
    for q in range(4):
        for k in range(GROUP):
            if k > 0 or q % 2 == 1:
                t_copy(q, k, homes[1]).wait_recv()
    got = tn(pick[...], home[...].reshape(n * 2 * slots, block))
    token_ref[...] = (got + back_dense).astype(BF)

    pltpu.make_async_copy(to_home.at[0], home_score.at[ep], local.at[2]).wait()
    for e in range(2):
        for i in range(n):
            if i > 0:
                a_copy(e, i, targets[i]).wait_send()
            o_copy(e, i).wait_send()
            for way in range(2):
                y_copy(e, i, way).wait_send()
                q_copy(e, i, way).wait_send()
    for i in range(1, n):
        w_copy(i).wait_send()
        k_copy(i).wait()
    for k in range(1, 8):
        score_copy(k).wait_send()
    for q in range(4):
        act_copy(q).wait()
        for j in range(4):
            d_copy(q, j).wait_send()
        for way in range(2):
            f_copy(q, way).wait_send()
            h_copy(q, way).wait_send()
        for k in range(GROUP):
            if k > 0 or q % 2 == 1:
                t_copy(q, k, homes[1]).wait_send()
    for e in range(2):
        held_copy(0, e).wait()
        held_copy(1, e).wait()


def exchange(rows, weights, wg, wu, wd, tokens, cotangent, scale, dw, pick):
    n, _, slots, half = rows.shape
    model, block, width = 2 * half, half // 4, dw.shape[1]
    tok_rows = tokens.shape[0]
    units = wg.shape[2]
    dma, vmem = pltpu.SemaphoreType.DMA, pltpu.VMEM
    many = GROUP * slots
    any_space, in_vmem = pl.BlockSpec(memory_space=pl.ANY), pl.BlockSpec(memory_space=vmem)
    return pl.pallas_call(
        functools.partial(exchange_kernel, n),
        out_shape=(
            jax.ShapeDtypeStruct((2, 2, n, slots, model), BF),
            jax.ShapeDtypeStruct((3, 4, many, units), BF),
            jax.ShapeDtypeStruct((tok_rows, block), BF),
            jax.ShapeDtypeStruct(weights.shape, F32),
            jax.ShapeDtypeStruct((block, width), F32),
        ),
        in_specs=[any_space] * 7 + [in_vmem] + [any_space] * 2,
        out_specs=[any_space, any_space, in_vmem, any_space, in_vmem],
        scratch_shapes=[
            vmem((2, 2, n, slots, model), BF),
            vmem(weights.shape, F32),
            vmem(wg.shape, BF),
            vmem(wu.shape, BF),
            vmem(wd.shape, BF),
            vmem((3, 4, many, units), BF),
            vmem((4, many, model), BF),
            vmem((4, many, half), BF),
            vmem((4, many, half), BF),
            vmem((2, 4, many, block // 2), BF),
            vmem((2, 4, many, block), BF),
            vmem((4, many, block), BF),
            vmem((n, 2, slots, block), BF),
            vmem((2 * n, 128), F32),
            vmem((8, 2 * n, 128), F32),
            vmem(weights.shape, F32),
            vmem((tok_rows, block), BF),
            vmem(cotangent.shape, BF),
            vmem(pick.shape, BF),
            vmem((block, model), BF),
            vmem((n, block, width), BF),
            vmem((block, model), BF),
            dma((2, n)), dma((2, n)), dma((n,)), dma((n,)), dma((n,)), dma((n,)), dma((n,)), dma((n,)),
            dma((2, 2, n)), dma((2, 2, n)), dma((2, n)), dma((2, n)), dma((2, 2, n)), dma((2, 2, n)),
            dma((4, 4)), dma((4, 4)), dma((2, 4)), dma((2, 4)), dma((2, 4)), dma((2, 4)),
            dma((4, GROUP)), dma((4, GROUP)), dma((8,)), dma((8,)), dma((n,)), dma((n,)),
            dma((10,)), dma((3,)), dma((3, 4)),
        ],
        compiler_params=pltpu.CompilerParams(collective_id=0, has_side_effects=True, vmem_limit_bytes=62 << 20),
    )(rows, weights, wg, wu, wd, tokens, cotangent, scale, dw, pick)


def gradient_kernel(x_ref, c_ref, act_ref, gate_ref, up_ref, down_ref):
    x, cotan = x_ref[0, 0], c_ref[0, 0]
    many = act_ref.shape[2] * act_ref.shape[1]
    hidden, gate_back, up_back = (act_ref[k].reshape(many, act_ref.shape[3]) for k in range(3))
    gate_ref[0] = tn(x, gate_back)
    up_ref[0] = tn(x, up_back)
    down_ref[0] = tn(hidden, cotan)


def gradients(held, act):
    _, experts, many, model = held.shape
    units = act.shape[3]
    chunk = model // 4
    return pl.pallas_call(
        gradient_kernel,
        grid=(experts, model // chunk),
        out_shape=(
            jax.ShapeDtypeStruct((experts, model, units), F32),
            jax.ShapeDtypeStruct((experts, model, units), F32),
            jax.ShapeDtypeStruct((experts, units, model), F32),
        ),
        in_specs=[
            pl.BlockSpec((1, 1, many, chunk), lambda e, k: (0, e, 0, k)),
            pl.BlockSpec((1, 1, many, chunk), lambda e, k: (1, e, 0, k)),
            pl.BlockSpec((3, 2, many // 2, units), lambda e, k: (0, e, 0, 0)),
        ],
        out_specs=[
            pl.BlockSpec((1, chunk, units), lambda e, k: (e, k, 0)),
            pl.BlockSpec((1, chunk, units), lambda e, k: (e, k, 0)),
            pl.BlockSpec((1, units, chunk), lambda e, k: (e, 0, k)),
        ],
    )(held, held, act)


def shards(
    tokens, cotangent, expert_ids, route_weights, gate_weight, up_weight, down_weight, dense_weight, dense_gate
):
    tok_rows, model = tokens.shape
    top_count = expert_ids.shape[1]
    local_count = gate_weight.shape[0]
    n = lax.axis_size("ep")
    experts = local_count * n
    slots = tok_rows * top_count * 3 // (2 * experts)
    half, block = model // 2, model // 8
    ep, tp, y, c = place()

    names = expert_ids.T[None] == jnp.arange(experts, dtype=jnp.int32)[:, None, None]
    member = jnp.sum(names.astype(F32), axis=1)
    weight_of = jnp.sum(jnp.where(names, route_weights.T[None].astype(F32), 0.0), axis=1)
    row_at = lax.broadcasted_iota(jnp.int32, (tok_rows, tok_rows), 0)
    col_at = lax.broadcasted_iota(jnp.int32, (tok_rows, tok_rows), 1)
    before = (row_at < col_at).astype(BF)
    rank = jnp.dot(member.astype(BF), before, preferred_element_type=F32)
    rank = jnp.where(member > 0.5, rank, -1.0)
    places = jnp.arange(slots, dtype=jnp.int32).astype(F32)
    picked = rank[:, None, :] == places[None, :, None]
    pick = picked.astype(BF)
    slot_weight = jnp.sum(jnp.where(picked, weight_of[:, None, :], 0.0), axis=2)
    pick_rows = pick.reshape(experts * slots, tok_rows)
    weights = jnp.pad(slot_weight.reshape(n, local_count, slots), ((0, 0), (0, 8 - local_count), (0, 128 - slots)))

    source = jnp.where(
        lax.rem(y, 2) == 0,
        lax.dynamic_slice_in_dim(tokens, c * half, half, 1),
        lax.dynamic_slice_in_dim(cotangent, c * half, half, 1),
    )
    rows = jnp.dot(pick_rows, source, preferred_element_type=F32).astype(BF)
    rows = rows.reshape(n, local_count, slots, half)

    held, act, token_grad, home_score, dense_grad = exchange(
        rows, weights, gate_weight, up_weight, down_weight, tokens, cotangent, dense_gate[None, :], dense_weight, pick_rows
    )
    grad_gate, grad_up, grad_down = gradients(held.reshape(2, local_count, n * slots, model), act)

    slot_score = home_score[:, :local_count, :slots].reshape(experts, slots, 1)
    of_expert = jnp.sum(jnp.where(picked, slot_score, 0.0), axis=1)
    of_choice = jnp.sum(jnp.where(names, of_expert[:, None, :], 0.0), axis=0)
    weight_grad = of_choice.T.astype(BF)
    return token_grad, weight_grad, grad_gate, grad_up, grad_down, dense_grad


def solution(mesh):
    in_specs = (
        P("ep", None),
        P("ep", None),
        P("ep", None),
        P("ep", None),
        P("ep", None, "tp"),
        P("ep", None, "tp"),
        P("ep", "tp", None),
        P("tp", "ep"),
        P(),
    )
    out_specs = (
        P("ep", "tp"),
        P("ep", None),
        P("ep", None, "tp"),
        P("ep", None, "tp"),
        P("ep", "tp", None),
        P("tp", "ep"),
    )
    return jax.shard_map(shards, mesh=mesh, in_specs=in_specs, out_specs=out_specs, check_vma=False)
```

```python
import functools

import jax
import jax.numpy as jnp
from jax import lax
from jax.experimental import pallas as pl
from jax.experimental.pallas import tpu as pltpu
from jax.sharding import PartitionSpec as P

clamp_limit = 7.0
sigmoid_slope = 1.702
MESH = pl.DeviceIdType.MESH
BF = jnp.bfloat16
F32 = jnp.float32
SIDE = 4
ORDER = (
    (0, 0), (0, 1), (1, 0), (0, 3), (3, 0), (1, 1), (3, 3), (1, 3),
    (3, 1), (0, 2), (2, 0), (2, 2), (1, 2), (2, 1), (3, 2), (2, 3),
)
GROUP = 4
LAG = 5
SLACK = 3


def place():
    ep, tp = lax.axis_index("ep"), lax.axis_index("tp")
    return ep, tp, tp // 2, lax.rem(tp, 2)


def shifted(ep, step, sign):
    z, x = ep // SIDE, lax.rem(ep, SIDE)
    dz, dx = step
    if sign < 0:
        dz, dx = SIDE - dz, SIDE - dx
    return lax.rem(z + dz, SIDE) * SIDE + lax.rem(x + dx, SIDE)


def tp_at(y, c):
    return lax.rem(y, 4) * 2 + c


def greet(devices):
    for device in devices:
        pl.semaphore_signal(pltpu.get_barrier_semaphore(), inc=1, device_id=device, device_id_type=MESH)


def remote(src, dst, send, recv, device):
    return pltpu.make_async_remote_copy(
        src_ref=src, dst_ref=dst, send_sem=send, recv_sem=recv, device_id=device, device_id_type=MESH
    )


def nn(a, b):
    return lax.dot_general(a, b, (((1,), (0,)), ((), ())), preferred_element_type=F32)


def nt(a, b):
    return lax.dot_general(a, b, (((1,), (1,)), ((), ())), preferred_element_type=F32)


def tn(a, b):
    return lax.dot_general(a, b, (((0,), (0,)), ((), ())), preferred_element_type=F32)


def exchange_kernel(
    n, slots, weight_ref, wg_ref, wu_ref, wd_ref, tok_ref, cot_ref, scale_ref, dw_ref, pick_ref,
    gate_out, up_out, down_out, token_ref, home_score, dense_out,
    sent, source, gate_sum, up_sum, down_sum, r, rw, wg, wu, wd, act, back, mine, part, first, second, total, home, score, scores, to_home,
    tok, cot, pick, dsend, dland, dwall,
    a_send, a_recv, w_send, w_recv, b_send, b_recv, g_send, g_recv,
    y_send, y_recv, o_send, o_recv, q_send, q_recv, d_send, d_recv, f_send, f_recv, h_send, h_recv,
    t_send, t_recv, s_send, s_recv, k_send, k_recv, load, local, out_sem,
):
    ep, tp, y, c = place()
    half = cot_ref.shape[1] // 2
    per = n // GROUP
    groups = 2 * per
    quarter, block, width = half // 2, half // 4, dw_ref.shape[1]
    rows = GROUP * slots
    par = lax.rem(y, 2)
    up, down, mate = (ep, tp_at(y + 1, c)), (ep, tp_at(y + 3, c)), (ep, tp_at(y, 1 - c))
    others = [(ep, lax.rem(tp + k, 8)) for k in range(1, 8)]
    targets = [shifted(ep, step, 1) for step in ORDER]
    homes = [shifted(ep, step, -1) for step in ORDER]

    def columns(start, size):
        return pl.ds(pl.multiple_of(start, 128), size)

    mine_cols = columns(c * half, half)
    ep_cols = columns(ep * width, width)

    greet([(targets[i], tp) for i in range(1, n)] + others)
    pick_load = pltpu.make_async_copy(pick_ref, pick, load.at[0])
    pick_load.start()
    token_part = pltpu.make_async_copy(tok_ref.at[:, mine_cols], source, load.at[1])
    cotan_part = pltpu.make_async_copy(cot_ref.at[:, mine_cols], source, load.at[1])

    @pl.when(par == 0)
    def _():
        token_part.start()

    @pl.when(par == 1)
    def _():
        cotan_part.start()

    loads = [
        pltpu.make_async_copy(a, b, load.at[2 + k])
        for k, (a, b) in enumerate(
            [
                (tok_ref.at[:, columns(tp * block, block)], tok),
                (cot_ref, cot),
                (wg_ref, wg),
                (wu_ref, wu),
                (wd_ref, wd),
                (dw_ref, dwall.at[:, ep_cols]),
                (weight_ref.at[ep], rw.at[0]),
            ]
        )
    ]
    for copy in loads:
        copy.start()
    pick_load.wait()
    token_part.wait()
    few = n // SIDE
    for k in range(SIDE):
        for m in range(2):
            cols = pl.ds(m * quarter, quarter)
            chosen = nn(pick[k * few * 2 * slots : (k + 1) * few * 2 * slots], source[:, cols])
            sent[k * few : (k + 1) * few, :, :, cols] = chosen.astype(BF).reshape(few, 2, slots, quarter)
    own_rows = [
        pltpu.make_async_copy(sent.at[ep, e], r.at[par, e, 0, :, mine_cols], load.at[9 + e]) for e in range(2)
    ]
    for copy in own_rows:
        copy.start()
    pl.semaphore_wait(pltpu.get_barrier_semaphore(), n - 1 + len(others))

    def a_copy(e, i, to):
        return remote(
            sent.at[to, e], r.at[par, e, i, :, mine_cols], a_send.at[e, i], a_recv.at[e, i], (to, tp)
        )

    def w_copy(i):
        return remote(weight_ref.at[targets[i]], rw.at[i], w_send.at[i], w_recv.at[i], (targets[i], tp))

    def b_copy(i):
        return remote(dw_ref, dwall.at[:, ep_cols], b_send.at[i], b_recv.at[i], (targets[i], tp))

    def g_copy(i):
        return remote(
            dsend.at[:, columns(targets[i] * width, width)], dland.at[i], g_send.at[i], g_recv.at[i], (targets[i], tp)
        )

    for i in range(1, n):
        w_copy(i).start()
    for e in range(2):
        for i in range(1, n):
            a_copy(e, i, targets[i]).start()
    for i in range(1, n):
        b_copy(i).start()

    loads[0].wait()
    loads[1].wait()
    cot[...] = (scale_ref[...] * cot[...].astype(F32)).astype(BF)
    for k in range(4):
        dsend[:, k * half // 2 : (k + 1) * half // 2] = tn(
            tok[...], cot[:, k * half // 2 : (k + 1) * half // 2]
        ).astype(BF)
    dland[0] = dsend[:, ep_cols]
    for i in range(1, n):
        g_copy(i).start()
    for copy in loads[2:] + own_rows:
        copy.wait()
    for i in range(1, n):
        w_copy(i).wait_recv()

    def y_copy(e, i, way):
        piece = r.at[par, e, i, :, columns(c * half + way * quarter, quarter)]
        return remote(piece, piece, y_send.at[way, e, i], y_recv.at[way, e, i], up if way == 0 else down)

    def o_copy(e, i):
        piece = r.at[par, e, i, :, mine_cols]
        return remote(piece, piece, o_send.at[e, i], o_recv.at[e, i], mate)

    def q_copy(e, i, way):
        piece = r.at[1 - par, e, i, :, columns(c * half + way * quarter, quarter)]
        return remote(piece, piece, q_send.at[way, e, i], q_recv.at[way, e, i], mate)

    def serve(t):
        @pl.when(t < 2 * n)
        def _():
            e, i = t // n, lax.rem(t, n)

            @pl.when(i > 0)
            def _():
                a_copy(e, i, targets[1]).wait_recv()

            y_copy(e, i, 0).start()
            y_copy(e, i, 1).start()
            o_copy(e, i).start()

        @pl.when(t >= LAG)
        def _():
            e, i = (t - LAG) // n, lax.rem(t - LAG, n)
            for way in range(2):
                y_copy(e, i, way).wait_recv()
                q_copy(e, i, way).start()

    def group(q):
        return q // per, pl.ds(lax.rem(q, per) * GROUP, GROUP)

    def ready(q):
        e = q // per

        @pl.loop(0, GROUP)
        def _(k):
            i = lax.rem(q, per) * GROUP + k
            o_copy(e, i).wait_recv()
            for way in range(2):
                q_copy(e, i, way).wait_recv()

    diagonal = lax.broadcasted_iota(jnp.int32, (slots, 128), 0) == lax.broadcasted_iota(jnp.int32, (slots, 128), 1)

    def expert_rows(q):
        e, who = group(q)
        x = r[0, e, who].reshape(rows, 2 * half)
        cotan = r[1, e, who].reshape(rows, 2 * half)
        gate_pre = nn(x, wg[e])
        up_pre = nn(x, wu[e])
        down_back = nt(cotan, wd[e])
        lanes = jnp.where(e == 0, rw[who, 0, :], rw[who, 1, :])
        weight = jnp.sum(jnp.where(diagonal[None], lanes[:, None, :], 0.0), axis=2, keepdims=True).reshape(rows, 1)
        gate_val = jnp.minimum(gate_pre, clamp_limit)
        up_val = jnp.clip(up_pre, -clamp_limit, clamp_limit)
        squash = jax.nn.sigmoid(sigmoid_slope * gate_val)
        swish = gate_val * squash
        hidden = ((up_val + 1.0) * swish).astype(BF).astype(F32)
        row_score = jnp.sum(hidden * down_back, axis=1, keepdims=True).reshape(GROUP, slots, 1)
        score[q] = jnp.sum(jnp.where(diagonal[None], row_score, 0.0), axis=1)
        hidden_back = weight * down_back
        slope = squash + sigmoid_slope * swish * (1.0 - squash)
        act[0, q] = (weight * hidden).astype(BF)
        act[1, q] = jnp.where(gate_pre < clamp_limit, hidden_back * (up_val + 1.0) * slope, 0.0).astype(BF)
        act[2, q] = jnp.where(jnp.abs(up_pre) < clamp_limit, hidden_back * swish, 0.0).astype(BF)
        for k in range(4):
            cols = pl.ds(k * half // 2, half // 2)
            value = nt(act[1, q], wg[e, cols, :]) + nt(act[2, q], wu[e, cols, :])
            back[q, :, cols] = value.astype(BF)

    def d_copy(q, j):
        return remote(
            back.at[q, :, columns((2 * j + 1 - c) * block, block)], mine.at[q, :, pl.ds(j * block, block)],
            d_send.at[j, q], d_recv.at[j, q], mate,
        )

    def f_copy(q, way):
        start = lax.rem(y + 2, 4) * block + way * (block // 2)
        return remote(
            part.at[q, :, columns(start, block // 2)], first.at[way, q], f_send.at[way, q], f_recv.at[way, q],
            up if way == 0 else down,
        )

    def h_copy(q, way):
        start = lax.rem(y + (1 if way == 0 else 3), 4) * block
        return remote(
            part.at[q, :, columns(start, block)], second.at[way, q], h_send.at[way, q], h_recv.at[way, q],
            up if way == 0 else down,
        )

    def t_copy(q, k, to):
        return remote(
            total.at[q, pl.ds(k * slots, slots)], home.at[ep, q // per], t_send.at[q, k], t_recv.at[q, k], (to, tp)
        )

    def own_total(e):
        return pltpu.make_async_copy(total.at[per * e, pl.ds(0, slots)], home.at[ep, e], local.at[e])

    def core_sum(q):
        for j in range(4):
            d_copy(q, j).wait_recv()
        for j in range(4):
            cols = pl.ds(j * block, block)
            both = back[q, :, columns((2 * j + c) * block, block)].astype(F32) + mine[q, :, cols].astype(F32)
            part[q, :, cols] = both.astype(BF)
        for way in range(2):
            f_copy(q, way).start()

    def ring_sum(q):
        for way in range(2):
            f_copy(q, way).wait_recv()
        for way in range(2):
            start = lax.rem(y + (1 if way == 0 else 3), 4) * block + way * (block // 2)
            cols = columns(start, block // 2)
            part[q, :, cols] = (part[q, :, cols].astype(F32) + first[way, q].astype(F32)).astype(BF)
        for way in range(2):
            h_copy(q, way).start()

    def home_sum(q):
        for way in range(2):
            h_copy(q, way).wait_recv()
        value = part[q, :, columns(y * block, block)].astype(F32)
        total[q] = (value + second[0, q].astype(F32) + second[1, q].astype(F32)).astype(BF)
        for k in range(GROUP):
            to = homes[k]
            for m in range(1, per):
                to = jnp.where(lax.rem(q, per) == m, homes[m * GROUP + k], to)
            if k == 0:

                @pl.when(lax.rem(q, per) == 0)
                def _():
                    own_total(q // per).start()

                @pl.when(lax.rem(q, per) > 0)
                def _(to=to):
                    t_copy(q, 0, to).start()

            else:
                t_copy(q, k, to).start()

    def sum_chunk(e, k):
        cols = pl.ds(pl.multiple_of(k * quarter, quarter), quarter)
        of_expert = pl.ds(e * per, per)
        x = r[0, e, :, :, cols].reshape(n * slots, quarter)
        cotan = r[1, e, :, :, cols].reshape(n * slots, quarter)
        hidden, gate_back, up_back = (act[a, of_expert].reshape(n * slots, act.shape[3]) for a in range(3))
        gate_sum[e, cols, :] = tn(x, gate_back).astype(BF)
        up_sum[e, cols, :] = tn(x, up_back).astype(BF)
        down_sum[e, :, cols] = tn(hidden, cotan).astype(BF)

    def sum_copies(e):
        pairs = [(gate_sum, gate_out), (up_sum, up_out), (down_sum, down_out)]
        return [pltpu.make_async_copy(a.at[e], b.at[e], out_sem.at[e, k]) for k, (a, b) in enumerate(pairs)]

    def score_copy(k):
        return remote(score, scores.at[tp], s_send.at[k], s_recv.at[k], (ep, lax.rem(tp + k, 8)))

    def k_copy(i):
        return remote(to_home.at[i], home_score.at[ep], k_send.at[i], k_recv.at[i], (homes[i], tp))

    @pl.loop(0, groups + 3)
    def _(q):
        last = 2 * n + LAG
        start = jnp.where(q == 0, 0, jnp.where(q >= groups, last, jnp.minimum(q * GROUP + LAG + SLACK, last)))
        stop = jnp.where(q >= groups - 1, last, jnp.minimum((q + 1) * GROUP + LAG + SLACK, last))
        pl.loop(start, stop)(serve)

        @pl.when((q >= 1) & (q < groups + 1))
        def _():
            core_sum(q - 1)

        @pl.when((q >= 2) & (q < groups + 2))
        def _():
            ring_sum(q - 2)

        @pl.when(q >= 3)
        def _():
            home_sum(q - 3)

        @pl.when(q < groups)
        def _():
            ready(q)
            expert_rows(q)
            for j in range(4):
                d_copy(q, j).start()

        @pl.when((q >= per) & (q < groups + 2))
        def _():
            chunk = jnp.where(q < groups, q - per, 2 * (q - groups))
            chunk_stop = jnp.where(q < groups, chunk + 1, chunk + 2)

            @pl.loop(chunk, chunk_stop)
            def _(k):
                sum_chunk(jnp.where(q < groups, 0, 1), k)

        @pl.when(q == groups - 1)
        def _():
            for copy in sum_copies(0):
                copy.start()
            for k in range(1, 8):
                score_copy(k).start()
            scores[tp] = score[...]

        @pl.when(q == groups + 1)
        def _():
            for copy in sum_copies(1):
                copy.start()
            for k in range(1, 8):
                score_copy(k).wait_recv()
            every = scores[0]
            for k in range(1, 8):
                every = every + scores[k]
            lower = lax.broadcasted_iota(jnp.int32, (8, 128), 0) == 0
            for i in range(n):
                g, k = i // GROUP, i % GROUP
                to_home[i] = jnp.where(lower, every[g, k : k + 1, :], every[per + g, k : k + 1, :])
            pltpu.make_async_copy(to_home.at[0], home_score.at[ep], local.at[2]).start()
            for i in range(1, n):
                k_copy(i).start()

    for i in range(1, n):
        b_copy(i).wait()
        g_copy(i).wait()
    dense = dland[0].astype(F32)
    for i in range(1, n):
        dense = dense + dland[i].astype(F32)
    dense_out[...] = dense
    back_dense = nt(cot[...], dwall[...])

    for e in range(2):
        for i in range(n):
            if i > 0:
                a_copy(e, i, targets[i]).wait_send()
            o_copy(e, i).wait_send()
            for way in range(2):
                y_copy(e, i, way).wait_send()
                q_copy(e, i, way).wait_send()
    for i in range(1, n):
        w_copy(i).wait_send()
    for k in range(1, 8):
        score_copy(k).wait_send()
    for q in range(groups):
        for j in range(4):
            d_copy(q, j).wait_send()
        for way in range(2):
            f_copy(q, way).wait_send()
            h_copy(q, way).wait_send()
    own_total(0).wait()
    own_total(1).wait()
    for q in range(groups):
        for k in range(GROUP):
            if k > 0 or q % per > 0:
                t_copy(q, k, homes[1]).wait_recv()
    got = tn(pick[...], home[...].reshape(n * 2 * slots, block))
    token_ref[...] = (got + back_dense).astype(BF)

    pltpu.make_async_copy(to_home.at[0], home_score.at[ep], local.at[2]).wait()
    for i in range(1, n):
        k_copy(i).wait()
    for q in range(groups):
        for k in range(GROUP):
            if k > 0 or q % per > 0:
                t_copy(q, k, homes[1]).wait_send()
    for e in range(2):
        for copy in sum_copies(e):
            copy.wait()


def exchange(weights, wg, wu, wd, tokens, cotangent, scale, dw, pick):
    n = weights.shape[0]
    slots = pick.shape[0] // (2 * n)
    tok_rows, model = tokens.shape
    half, block, width = model // 2, model // 8, dw.shape[1]
    units = wg.shape[2]
    dma, vmem = pltpu.SemaphoreType.DMA, pltpu.VMEM
    many, groups = GROUP * slots, 2 * n // GROUP
    any_space, in_vmem = pl.BlockSpec(memory_space=pl.ANY), pl.BlockSpec(memory_space=vmem)
    return pl.pallas_call(
        functools.partial(exchange_kernel, n, slots),
        out_shape=(
            jax.ShapeDtypeStruct(wg.shape, BF),
            jax.ShapeDtypeStruct(wu.shape, BF),
            jax.ShapeDtypeStruct(wd.shape, BF),
            jax.ShapeDtypeStruct((tok_rows, block), BF),
            jax.ShapeDtypeStruct(weights.shape, F32),
            jax.ShapeDtypeStruct((block, width), F32),
        ),
        in_specs=[any_space] * 6 + [in_vmem] + [any_space] * 2,
        out_specs=[any_space, any_space, any_space, in_vmem, any_space, in_vmem],
        scratch_shapes=[
            vmem((n, 2, slots, half), BF),
            vmem((tok_rows, half), BF),
            vmem(wg.shape, BF),
            vmem(wu.shape, BF),
            vmem(wd.shape, BF),
            vmem((2, 2, n, slots, model), BF),
            vmem(weights.shape, F32),
            vmem(wg.shape, BF),
            vmem(wu.shape, BF),
            vmem(wd.shape, BF),
            vmem((3, groups, many, units), BF),
            vmem((groups, many, model), BF),
            vmem((groups, many, half), BF),
            vmem((groups, many, half), BF),
            vmem((2, groups, many, block // 2), BF),
            vmem((2, groups, many, block), BF),
            vmem((groups, many, block), BF),
            vmem((n, 2, slots, block), BF),
            vmem((groups, GROUP, 128), F32),
            vmem((8, groups, GROUP, 128), F32),
            vmem(weights.shape, F32),
            vmem((tok_rows, block), BF),
            vmem(cotangent.shape, BF),
            vmem(pick.shape, BF),
            vmem((block, model), BF),
            vmem((n, block, width), BF),
            vmem((block, model), BF),
            dma((2, n)), dma((2, n)), dma((n,)), dma((n,)), dma((n,)), dma((n,)), dma((n,)), dma((n,)),
            dma((2, 2, n)), dma((2, 2, n)), dma((2, n)), dma((2, n)), dma((2, 2, n)), dma((2, 2, n)),
            dma((4, groups)), dma((4, groups)), dma((2, groups)), dma((2, groups)), dma((2, groups)), dma((2, groups)),
            dma((groups, GROUP)), dma((groups, GROUP)), dma((8,)), dma((8,)), dma((n,)), dma((n,)),
            dma((11,)), dma((3,)), dma((2, 3)),
        ],
        compiler_params=pltpu.CompilerParams(collective_id=0, has_side_effects=True, vmem_limit_bytes=63 << 20),
    )(weights, wg, wu, wd, tokens, cotangent, scale, dw, pick)


def shards(
    tokens, cotangent, expert_ids, route_weights, gate_weight, up_weight, down_weight, dense_weight, dense_gate
):
    tok_rows, model = tokens.shape
    top_count = expert_ids.shape[1]
    local_count = gate_weight.shape[0]
    n = lax.axis_size("ep")
    experts = local_count * n
    slots = tok_rows * top_count * 3 // (2 * experts)
    names = expert_ids.T[None] == jnp.arange(experts, dtype=jnp.int32)[:, None, None]
    member = jnp.sum(names.astype(F32), axis=1)
    weight_of = jnp.sum(jnp.where(names, route_weights.T[None].astype(F32), 0.0), axis=1)
    row_at = lax.broadcasted_iota(jnp.int32, (tok_rows, tok_rows), 0)
    col_at = lax.broadcasted_iota(jnp.int32, (tok_rows, tok_rows), 1)
    before = (row_at < col_at).astype(BF)
    rank = jnp.dot(member.astype(BF), before, preferred_element_type=F32)
    rank = jnp.where(member > 0.5, rank, -1.0)
    places = jnp.arange(slots, dtype=jnp.int32).astype(F32)
    picked = rank[:, None, :] == places[None, :, None]
    pick = picked.astype(BF)
    slot_weight = jnp.sum(jnp.where(picked, weight_of[:, None, :], 0.0), axis=2)
    pick_rows = pick.reshape(experts * slots, tok_rows)
    weights = jnp.pad(slot_weight.reshape(n, local_count, slots), ((0, 0), (0, 8 - local_count), (0, 128 - slots)))

    grad_gate, grad_up, grad_down, token_grad, home_score, dense_grad = exchange(
        weights, gate_weight, up_weight, down_weight, tokens, cotangent, dense_gate[None, :], dense_weight, pick_rows
    )

    slot_score = home_score[:, :local_count, :slots].reshape(experts, slots, 1)
    of_expert = jnp.sum(jnp.where(picked, slot_score, 0.0), axis=1)
    of_choice = jnp.sum(jnp.where(names, of_expert[:, None, :], 0.0), axis=0)
    weight_grad = of_choice.T.astype(BF)
    return (
        token_grad,
        weight_grad,
        grad_gate.astype(F32),
        grad_up.astype(F32),
        grad_down.astype(F32),
        dense_grad,
    )


def solution(mesh):
    in_specs = (
        P("ep", None),
        P("ep", None),
        P("ep", None),
        P("ep", None),
        P("ep", None, "tp"),
        P("ep", None, "tp"),
        P("ep", "tp", None),
        P("tp", "ep"),
        P(),
    )
    out_specs = (
        P("ep", "tp"),
        P("ep", None),
        P("ep", None, "tp"),
        P("ep", None, "tp"),
        P("ep", "tp", None),
        P("tp", "ep"),
    )
    return jax.shard_map(shards, mesh=mesh, in_specs=in_specs, out_specs=out_specs, check_vma=False)
```

```python
import functools

import jax
import jax.numpy as jnp
from jax import lax
from jax.experimental import pallas as pl
from jax.experimental.pallas import tpu as pltpu
from jax.sharding import PartitionSpec as P

clamp_limit = 7.0
sigmoid_slope = 1.702
MESH = pl.DeviceIdType.MESH
BF = jnp.bfloat16
F32 = jnp.float32
SIDE = 4
ORDER = (
    (0, 0), (0, 1), (1, 0), (0, 3), (3, 0), (1, 1), (3, 3), (1, 3),
    (3, 1), (0, 2), (2, 0), (2, 2), (1, 2), (2, 1), (3, 2), (2, 3),
)
GROUP = 4
LAG = 5
SLACK = 3


def place():
    ep, tp = lax.axis_index("ep"), lax.axis_index("tp")
    return ep, tp, tp // 2, lax.rem(tp, 2)


def shifted(ep, step, sign):
    z, x = ep // SIDE, lax.rem(ep, SIDE)
    dz, dx = step
    if sign < 0:
        dz, dx = SIDE - dz, SIDE - dx
    return lax.rem(z + dz, SIDE) * SIDE + lax.rem(x + dx, SIDE)


def tp_at(y, c):
    return lax.rem(y, 4) * 2 + c


def greet(devices):
    for device in devices:
        pl.semaphore_signal(pltpu.get_barrier_semaphore(), inc=1, device_id=device, device_id_type=MESH)


def remote(src, dst, send, recv, device):
    return pltpu.make_async_remote_copy(
        src_ref=src, dst_ref=dst, send_sem=send, recv_sem=recv, device_id=device, device_id_type=MESH
    )


def nn(a, b):
    return lax.dot_general(a, b, (((1,), (0,)), ((), ())), preferred_element_type=F32)


def nt(a, b):
    return lax.dot_general(a, b, (((1,), (1,)), ((), ())), preferred_element_type=F32)


def tn(a, b):
    return lax.dot_general(a, b, (((0,), (0,)), ((), ())), preferred_element_type=F32)


def exchange_kernel(
    n, slots, weight_ref, wg_ref, wu_ref, wd_ref, tok_ref, cot_ref, scale_ref, dw_ref, pick_ref,
    gate_out, up_out, down_out, token_ref, home_score, dense_out,
    sent, source, gate_sum, up_sum, down_sum, r, rw, wg, wu, wd, act, back, mine, part, first, second, total, home, score, scores, to_home,
    tok, cot, pick, dsend, dland, dwall,
    a_send, a_recv, w_send, w_recv, b_send, b_recv, g_send, g_recv,
    y_send, y_recv, o_send, o_recv, q_send, q_recv, d_send, d_recv, f_send, f_recv, h_send, h_recv,
    t_send, t_recv, s_send, s_recv, k_send, k_recv, load, local, out_sem,
):
    ep, tp, y, c = place()
    half = cot_ref.shape[1] // 2
    per = n // GROUP
    groups = 2 * per
    quarter, block, width = half // 2, half // 4, dw_ref.shape[1]
    rows = GROUP * slots
    par = lax.rem(y, 2)
    up, down, mate = (ep, tp_at(y + 1, c)), (ep, tp_at(y + 3, c)), (ep, tp_at(y, 1 - c))
    others = [(ep, lax.rem(tp + k, 8)) for k in range(1, 8)]
    targets = [shifted(ep, step, 1) for step in ORDER]
    homes = [shifted(ep, step, -1) for step in ORDER]

    def columns(start, size):
        return pl.ds(pl.multiple_of(start, 128), size)

    mine_cols = columns(c * half, half)
    ep_cols = columns(ep * width, width)

    greet([(targets[i], tp) for i in range(1, n)] + others)
    pick_load = pltpu.make_async_copy(pick_ref, pick, load.at[0])
    pick_load.start()
    token_part = pltpu.make_async_copy(tok_ref.at[:, mine_cols], source, load.at[1])
    cotan_part = pltpu.make_async_copy(cot_ref.at[:, mine_cols], source, load.at[1])

    @pl.when(par == 0)
    def _():
        token_part.start()

    @pl.when(par == 1)
    def _():
        cotan_part.start()

    loads = [
        pltpu.make_async_copy(a, b, load.at[2 + k])
        for k, (a, b) in enumerate(
            [
                (tok_ref.at[:, columns(tp * block, block)], tok),
                (cot_ref, cot),
                (wg_ref, wg),
                (wu_ref, wu),
                (wd_ref, wd),
                (dw_ref, dwall.at[:, ep_cols]),
                (weight_ref.at[ep], rw.at[0]),
            ]
        )
    ]
    for copy in loads:
        copy.start()
    pick_load.wait()
    token_part.wait()
    few = n // SIDE
    for k in range(SIDE):
        for m in range(2):
            cols = pl.ds(m * quarter, quarter)
            chosen = nn(pick[k * few * 2 * slots : (k + 1) * few * 2 * slots], source[:, cols])
            sent[k * few : (k + 1) * few, :, :, cols] = chosen.astype(BF).reshape(few, 2, slots, quarter)
    own_rows = [
        pltpu.make_async_copy(sent.at[ep, e], r.at[par, e, 0, :, mine_cols], load.at[9 + e]) for e in range(2)
    ]
    for copy in own_rows:
        copy.start()
    pl.semaphore_wait(pltpu.get_barrier_semaphore(), n - 1 + len(others))

    def a_copy(e, i, to):
        return remote(
            sent.at[to, e], r.at[par, e, i, :, mine_cols], a_send.at[e, i], a_recv.at[e, i], (to, tp)
        )

    def w_copy(i):
        return remote(weight_ref.at[targets[i]], rw.at[i], w_send.at[i], w_recv.at[i], (targets[i], tp))

    def b_copy(i):
        return remote(dw_ref, dwall.at[:, ep_cols], b_send.at[i], b_recv.at[i], (targets[i], tp))

    def g_copy(i):
        return remote(
            dsend.at[:, columns(targets[i] * width, width)], dland.at[i], g_send.at[i], g_recv.at[i], (targets[i], tp)
        )

    for i in range(1, n):
        w_copy(i).start()
    for e in range(2):
        for i in range(1, n):
            a_copy(e, i, targets[i]).start()
    for i in range(1, n):
        b_copy(i).start()

    loads[0].wait()
    loads[1].wait()
    cot[...] = (scale_ref[...] * cot[...].astype(F32)).astype(BF)
    for k in range(4):
        dsend[:, k * half // 2 : (k + 1) * half // 2] = tn(
            tok[...], cot[:, k * half // 2 : (k + 1) * half // 2]
        ).astype(BF)
    dland[0] = dsend[:, ep_cols]
    for i in range(1, n):
        g_copy(i).start()
    for copy in loads[2:] + own_rows:
        copy.wait()
    for i in range(1, n):
        w_copy(i).wait_recv()

    def y_copy(e, i, way):
        piece = r.at[par, e, i, :, columns(c * half + way * quarter, quarter)]
        return remote(piece, piece, y_send.at[way, e, i], y_recv.at[way, e, i], up if way == 0 else down)

    def o_copy(e, i):
        piece = r.at[par, e, i, :, mine_cols]
        return remote(piece, piece, o_send.at[e, i], o_recv.at[e, i], mate)

    def q_copy(e, i, way):
        piece = r.at[1 - par, e, i, :, columns(c * half + way * quarter, quarter)]
        return remote(piece, piece, q_send.at[way, e, i], q_recv.at[way, e, i], mate)

    def serve(t):
        @pl.when(t < 2 * n)
        def _():
            e, i = t // n, lax.rem(t, n)

            @pl.when(i > 0)
            def _():
                a_copy(e, i, targets[1]).wait_recv()

            y_copy(e, i, 0).start()
            y_copy(e, i, 1).start()
            o_copy(e, i).start()

        @pl.when(t >= LAG)
        def _():
            e, i = (t - LAG) // n, lax.rem(t - LAG, n)
            for way in range(2):
                y_copy(e, i, way).wait_recv()
                q_copy(e, i, way).start()

    def group(q):
        return q // per, pl.ds(lax.rem(q, per) * GROUP, GROUP)

    def ready(q):
        e = q // per

        @pl.loop(0, GROUP)
        def _(k):
            i = lax.rem(q, per) * GROUP + k
            o_copy(e, i).wait_recv()
            for way in range(2):
                q_copy(e, i, way).wait_recv()

    diagonal = lax.broadcasted_iota(jnp.int32, (slots, 128), 0) == lax.broadcasted_iota(jnp.int32, (slots, 128), 1)

    def expert_rows(q):
        e, who = group(q)
        x = r[0, e, who].reshape(rows, 2 * half)
        cotan = r[1, e, who].reshape(rows, 2 * half)
        gate_pre = nn(x, wg[e])
        up_pre = nn(x, wu[e])
        down_back = nt(cotan, wd[e])
        lanes = jnp.where(e == 0, rw[who, 0, :], rw[who, 1, :])
        weight = jnp.sum(jnp.where(diagonal[None], lanes[:, None, :], 0.0), axis=2, keepdims=True).reshape(rows, 1)
        gate_val = jnp.minimum(gate_pre, clamp_limit)
        up_val = jnp.clip(up_pre, -clamp_limit, clamp_limit)
        squash = jax.nn.sigmoid(sigmoid_slope * gate_val)
        swish = gate_val * squash
        hidden = ((up_val + 1.0) * swish).astype(BF).astype(F32)
        row_score = jnp.sum(hidden * down_back, axis=1, keepdims=True).reshape(GROUP, slots, 1)
        score[q] = jnp.sum(jnp.where(diagonal[None], row_score, 0.0), axis=1)
        hidden_back = weight * down_back
        slope = squash + sigmoid_slope * swish * (1.0 - squash)
        act[0, q] = (weight * hidden).astype(BF)
        act[1, q] = jnp.where(gate_pre < clamp_limit, hidden_back * (up_val + 1.0) * slope, 0.0).astype(BF)
        act[2, q] = jnp.where(jnp.abs(up_pre) < clamp_limit, hidden_back * swish, 0.0).astype(BF)
        for k in range(4):
            cols = pl.ds(k * half // 2, half // 2)
            value = nt(act[1, q], wg[e, cols, :]) + nt(act[2, q], wu[e, cols, :])
            back[q, :, cols] = value.astype(BF)

    def d_copy(q, j):
        return remote(
            back.at[q, :, columns((2 * j + 1 - c) * block, block)], mine.at[q, :, pl.ds(j * block, block)],
            d_send.at[j, q], d_recv.at[j, q], mate,
        )

    def f_copy(q, way):
        start = lax.rem(y + 2, 4) * block + way * (block // 2)
        return remote(
            part.at[q, :, columns(start, block // 2)], first.at[way, q], f_send.at[way, q], f_recv.at[way, q],
            up if way == 0 else down,
        )

    def h_copy(q, way):
        start = lax.rem(y + (1 if way == 0 else 3), 4) * block
        return remote(
            part.at[q, :, columns(start, block)], second.at[way, q], h_send.at[way, q], h_recv.at[way, q],
            up if way == 0 else down,
        )

    def t_copy(q, k, to):
        return remote(
            total.at[q, pl.ds(k * slots, slots)], home.at[ep, q // per], t_send.at[q, k], t_recv.at[q, k], (to, tp)
        )

    def own_total(e):
        return pltpu.make_async_copy(total.at[per * e, pl.ds(0, slots)], home.at[ep, e], local.at[e])

    def core_sum(q):
        for j in range(4):
            d_copy(q, j).wait_recv()
        for j in range(4):
            cols = pl.ds(j * block, block)
            both = back[q, :, columns((2 * j + c) * block, block)].astype(F32) + mine[q, :, cols].astype(F32)
            part[q, :, cols] = both.astype(BF)
        for way in range(2):
            f_copy(q, way).start()

    def ring_sum(q):
        for way in range(2):
            f_copy(q, way).wait_recv()
        for way in range(2):
            start = lax.rem(y + (1 if way == 0 else 3), 4) * block + way * (block // 2)
            cols = columns(start, block // 2)
            part[q, :, cols] = (part[q, :, cols].astype(F32) + first[way, q].astype(F32)).astype(BF)
        for way in range(2):
            h_copy(q, way).start()

    def home_sum(q):
        for way in range(2):
            h_copy(q, way).wait_recv()
        value = part[q, :, columns(y * block, block)].astype(F32)
        total[q] = (value + second[0, q].astype(F32) + second[1, q].astype(F32)).astype(BF)
        for k in range(GROUP):
            to = homes[k]
            for m in range(1, per):
                to = jnp.where(lax.rem(q, per) == m, homes[m * GROUP + k], to)
            if k == 0:

                @pl.when(lax.rem(q, per) == 0)
                def _():
                    own_total(q // per).start()

                @pl.when(lax.rem(q, per) > 0)
                def _(to=to):
                    t_copy(q, 0, to).start()

            else:
                t_copy(q, k, to).start()

    def sum_chunk(e, k):
        cols = pl.ds(pl.multiple_of(k * quarter, quarter), quarter)
        of_expert = pl.ds(e * per, per)
        x = r[0, e, :, :, cols].reshape(n * slots, quarter)
        cotan = r[1, e, :, :, cols].reshape(n * slots, quarter)
        hidden, gate_back, up_back = (act[a, of_expert].reshape(n * slots, act.shape[3]) for a in range(3))
        gate_sum[e, cols, :] = tn(x, gate_back).astype(BF)
        up_sum[e, cols, :] = tn(x, up_back).astype(BF)
        down_sum[e, :, cols] = tn(hidden, cotan).astype(BF)

    def sum_copies(e):
        pairs = [(gate_sum, gate_out), (up_sum, up_out), (down_sum, down_out)]
        return [pltpu.make_async_copy(a.at[e], b.at[e], out_sem.at[e, k]) for k, (a, b) in enumerate(pairs)]

    def score_copy(k):
        return remote(score, scores.at[tp], s_send.at[k], s_recv.at[k], (ep, lax.rem(tp + k, 8)))

    def k_copy(i):
        return remote(to_home.at[i], home_score.at[ep], k_send.at[i], k_recv.at[i], (homes[i], tp))

    @pl.loop(0, groups + 5)
    def _(q):
        last = 2 * n + LAG
        start = jnp.where(q == 0, 0, jnp.where(q >= groups, last, jnp.minimum(q * GROUP + LAG + SLACK, last)))
        stop = jnp.where(q >= groups - 1, last, jnp.minimum((q + 1) * GROUP + LAG + SLACK, last))
        pl.loop(start, stop)(serve)

        @pl.when((q >= 1) & (q < groups + 1))
        def _():
            core_sum(q - 1)

        @pl.when((q >= 3) & (q < groups + 3))
        def _():
            ring_sum(q - 3)

        @pl.when(q >= 5)
        def _():
            home_sum(q - 5)

        @pl.when(q < groups)
        def _():
            ready(q)
            expert_rows(q)
            for j in range(4):
                d_copy(q, j).start()

        @pl.when((q >= per) & (q < groups + 2))
        def _():
            chunk = jnp.where(q < groups, q - per, 2 * (q - groups))
            chunk_stop = jnp.where(q < groups, chunk + 1, chunk + 2)

            @pl.loop(chunk, chunk_stop)
            def _(k):
                sum_chunk(jnp.where(q < groups, 0, 1), k)

        @pl.when(q == groups - 1)
        def _():
            for copy in sum_copies(0):
                copy.start()
            for k in range(1, 8):
                score_copy(k).start()
            scores[tp] = score[...]

        @pl.when(q == groups + 1)
        def _():
            for copy in sum_copies(1):
                copy.start()
            for k in range(1, 8):
                score_copy(k).wait_recv()
            every = scores[0]
            for k in range(1, 8):
                every = every + scores[k]
            lower = lax.broadcasted_iota(jnp.int32, (8, 128), 0) == 0
            for i in range(n):
                g, k = i // GROUP, i % GROUP
                to_home[i] = jnp.where(lower, every[g, k : k + 1, :], every[per + g, k : k + 1, :])
            pltpu.make_async_copy(to_home.at[0], home_score.at[ep], local.at[2]).start()
            for i in range(1, n):
                k_copy(i).start()

    for i in range(1, n):
        b_copy(i).wait()
        g_copy(i).wait()
    dense = dland[0].astype(F32)
    for i in range(1, n):
        dense = dense + dland[i].astype(F32)
    dense_out[...] = dense
    back_dense = nt(cot[...], dwall[...])

    for e in range(2):
        for i in range(n):
            if i > 0:
                a_copy(e, i, targets[i]).wait_send()
            o_copy(e, i).wait_send()
            for way in range(2):
                y_copy(e, i, way).wait_send()
                q_copy(e, i, way).wait_send()
    for i in range(1, n):
        w_copy(i).wait_send()
    for k in range(1, 8):
        score_copy(k).wait_send()
    for q in range(groups):
        for j in range(4):
            d_copy(q, j).wait_send()
        for way in range(2):
            f_copy(q, way).wait_send()
            h_copy(q, way).wait_send()
    own_total(0).wait()
    own_total(1).wait()
    for q in range(groups):
        for k in range(GROUP):
            if k > 0 or q % per > 0:
                t_copy(q, k, homes[1]).wait_recv()
    got = tn(pick[...], home[...].reshape(n * 2 * slots, block))
    token_ref[...] = (got + back_dense).astype(BF)

    pltpu.make_async_copy(to_home.at[0], home_score.at[ep], local.at[2]).wait()
    for i in range(1, n):
        k_copy(i).wait()
    for q in range(groups):
        for k in range(GROUP):
            if k > 0 or q % per > 0:
                t_copy(q, k, homes[1]).wait_send()
    for e in range(2):
        for copy in sum_copies(e):
            copy.wait()


def exchange(weights, wg, wu, wd, tokens, cotangent, scale, dw, pick):
    n = weights.shape[0]
    slots = pick.shape[0] // (2 * n)
    tok_rows, model = tokens.shape
    half, block, width = model // 2, model // 8, dw.shape[1]
    units = wg.shape[2]
    dma, vmem = pltpu.SemaphoreType.DMA, pltpu.VMEM
    many, groups = GROUP * slots, 2 * n // GROUP
    any_space, in_vmem = pl.BlockSpec(memory_space=pl.ANY), pl.BlockSpec(memory_space=vmem)
    return pl.pallas_call(
        functools.partial(exchange_kernel, n, slots),
        out_shape=(
            jax.ShapeDtypeStruct(wg.shape, BF),
            jax.ShapeDtypeStruct(wu.shape, BF),
            jax.ShapeDtypeStruct(wd.shape, BF),
            jax.ShapeDtypeStruct((tok_rows, block), BF),
            jax.ShapeDtypeStruct(weights.shape, F32),
            jax.ShapeDtypeStruct((block, width), F32),
        ),
        in_specs=[any_space] * 6 + [in_vmem] + [any_space] * 2,
        out_specs=[any_space, any_space, any_space, in_vmem, any_space, in_vmem],
        scratch_shapes=[
            vmem((n, 2, slots, half), BF),
            vmem((tok_rows, half), BF),
            vmem(wg.shape, BF),
            vmem(wu.shape, BF),
            vmem(wd.shape, BF),
            vmem((2, 2, n, slots, model), BF),
            vmem(weights.shape, F32),
            vmem(wg.shape, BF),
            vmem(wu.shape, BF),
            vmem(wd.shape, BF),
            vmem((3, groups, many, units), BF),
            vmem((groups, many, model), BF),
            vmem((groups, many, half), BF),
            vmem((groups, many, half), BF),
            vmem((2, groups, many, block // 2), BF),
            vmem((2, groups, many, block), BF),
            vmem((groups, many, block), BF),
            vmem((n, 2, slots, block), BF),
            vmem((groups, GROUP, 128), F32),
            vmem((8, groups, GROUP, 128), F32),
            vmem(weights.shape, F32),
            vmem((tok_rows, block), BF),
            vmem(cotangent.shape, BF),
            vmem(pick.shape, BF),
            vmem((block, model), BF),
            vmem((n, block, width), BF),
            vmem((block, model), BF),
            dma((2, n)), dma((2, n)), dma((n,)), dma((n,)), dma((n,)), dma((n,)), dma((n,)), dma((n,)),
            dma((2, 2, n)), dma((2, 2, n)), dma((2, n)), dma((2, n)), dma((2, 2, n)), dma((2, 2, n)),
            dma((4, groups)), dma((4, groups)), dma((2, groups)), dma((2, groups)), dma((2, groups)), dma((2, groups)),
            dma((groups, GROUP)), dma((groups, GROUP)), dma((8,)), dma((8,)), dma((n,)), dma((n,)),
            dma((11,)), dma((3,)), dma((2, 3)),
        ],
        compiler_params=pltpu.CompilerParams(collective_id=0, has_side_effects=True, vmem_limit_bytes=63 << 20),
    )(weights, wg, wu, wd, tokens, cotangent, scale, dw, pick)


def shards(
    tokens, cotangent, expert_ids, route_weights, gate_weight, up_weight, down_weight, dense_weight, dense_gate
):
    tok_rows, model = tokens.shape
    top_count = expert_ids.shape[1]
    local_count = gate_weight.shape[0]
    n = lax.axis_size("ep")
    experts = local_count * n
    slots = tok_rows * top_count * 3 // (2 * experts)
    names = expert_ids.T[None] == jnp.arange(experts, dtype=jnp.int32)[:, None, None]
    member = jnp.sum(names.astype(F32), axis=1)
    weight_of = jnp.sum(jnp.where(names, route_weights.T[None].astype(F32), 0.0), axis=1)
    row_at = lax.broadcasted_iota(jnp.int32, (tok_rows, tok_rows), 0)
    col_at = lax.broadcasted_iota(jnp.int32, (tok_rows, tok_rows), 1)
    before = (row_at < col_at).astype(BF)
    rank = jnp.dot(member.astype(BF), before, preferred_element_type=F32)
    rank = jnp.where(member > 0.5, rank, -1.0)
    places = jnp.arange(slots, dtype=jnp.int32).astype(F32)
    picked = rank[:, None, :] == places[None, :, None]
    pick = picked.astype(BF)
    slot_weight = jnp.sum(jnp.where(picked, weight_of[:, None, :], 0.0), axis=2)
    pick_rows = pick.reshape(experts * slots, tok_rows)
    weights = jnp.pad(slot_weight.reshape(n, local_count, slots), ((0, 0), (0, 8 - local_count), (0, 128 - slots)))

    grad_gate, grad_up, grad_down, token_grad, home_score, dense_grad = exchange(
        weights, gate_weight, up_weight, down_weight, tokens, cotangent, dense_gate[None, :], dense_weight, pick_rows
    )

    slot_score = home_score[:, :local_count, :slots].reshape(experts, slots, 1)
    of_expert = jnp.sum(jnp.where(picked, slot_score, 0.0), axis=1)
    of_choice = jnp.sum(jnp.where(names, of_expert[:, None, :], 0.0), axis=0)
    weight_grad = of_choice.T.astype(BF)
    return (
        token_grad,
        weight_grad,
        grad_gate.astype(F32),
        grad_up.astype(F32),
        grad_down.astype(F32),
        dense_grad,
    )


def solution(mesh):
    in_specs = (
        P("ep", None),
        P("ep", None),
        P("ep", None),
        P("ep", None),
        P("ep", None, "tp"),
        P("ep", None, "tp"),
        P("ep", "tp", None),
        P("tp", "ep"),
        P(),
    )
    out_specs = (
        P("ep", "tp"),
        P("ep", None),
        P("ep", None, "tp"),
        P("ep", None, "tp"),
        P("ep", "tp", None),
        P("tp", "ep"),
    )
    return jax.shard_map(shards, mesh=mesh, in_specs=in_specs, out_specs=out_specs, check_vma=False)
```
